128 devices in a mesh: sp: 16 (over z, x), tp: 8 (over y, core).
Axes of the slice: x: 4, y: 4, z: 4, core: 2. Of those that a mesh axis runs over, the one named last changes fastest.
Arguments:
- residual: bfloat16 [8192, 2048], P(('sp', 'tp')), may hold values from -6 to 6
- query_small: bfloat16 [8192, 8, 128], P('sp', 'tp'), may hold values from -120 to 120
- key_small: bfloat16 [8192, 8, 128], P('sp', 'tp'), may hold values from -6 to 6
- value_small: bfloat16 [8192, 8, 128], P('sp', 'tp'), may hold values from -6 to 6
- query_large: bfloat16 [8192, 8, 256], P('sp', 'tp'), may hold values from -120 to 120
- key_large: bfloat16 [8192, 8, 256], P('sp', 'tp'), may hold values from -6 to 6
- value_large: bfloat16 [8192, 8, 128], P('sp', 'tp'), may hold values from -6 to 6
- lambda_small: float32 [8], P('tp'), may hold values from 0.3 to 0.8
- lambda_large: float32 [8], P('tp'), may hold values from 0.3 to 0.8
- head_gain: float32 [128], replicated, may hold values from 0.1 to 1.9
- output_small: bfloat16 [1024, 2048], P('tp'), may hold values from -0.125 to 0.125
- output_large: bfloat16 [1024, 2048], P('tp'), may hold values from -0.125 to 0.125
- norm_gain: float32 [2048], replicated, may hold values from 0.1 to 1.9
- gate_weight: bfloat16 [2048, 5632], P('sp', 'tp'), may hold values from -0.125 to 0.125
- up_weight: bfloat16 [2048, 5632], P('sp', 'tp'), may hold values from -0.125 to 0.125
- down_weight: bfloat16 [5632, 2048], P('tp', 'sp'), may hold values from -0.3125 to 0.3125
Outputs:
- block_output: bfloat16 [8192, 2048], P(('sp', 'tp'))
The draws below stay inside these ranges and needn't reach their ends.
All inputs are finite; a program needn't handle non-finite values.
Results may differ from the reference program's by a relative error of at most 0.015.
Values may be sent and summed in bfloat16 or wider, within the bound.
A program may use at most 128 MiB of HBM per device.

```python
import math
import jax
import jax.numpy as jnp
from jax import lax

D = 2048
HA = 8
HB = 8
KA = 64
KB = 128
VD = 128
FF = 5632
SEQ = 8192


def draw_pair(key, head_count, width, salt):
    base = jax.random.fold_in(key, salt)
    key_draw, query_draw = jax.random.split(base, 2)
    key_rows = jnp.clip(1.3 * jax.random.normal(key_draw, (SEQ, head_count, width), jnp.float32), -6.0, 6.0)
    query_rows = jnp.clip(1.3 * jax.random.normal(query_draw, (SEQ, head_count, width), jnp.float32), -6.0, 6.0)
    return (query_rows, key_rows)


def draw_query_small(key, part):
    return draw_pair(key, HA, 2 * KA, 11)[0].astype(jnp.bfloat16)


def draw_key_small(key, part):
    return draw_pair(key, HA, 2 * KA, 11)[1].astype(jnp.bfloat16)


def draw_query_large(key, part):
    return draw_pair(key, HB, 2 * KB, 23)[0].astype(jnp.bfloat16)


def draw_key_large(key, part):
    return draw_pair(key, HB, 2 * KB, 23)[1].astype(jnp.bfloat16)


def block_levels(key, shape, shards, least, largest):
    def one(position, blocks):
        heights = jax.random.uniform(jax.random.fold_in(jax.random.fold_in(key, 6), position), (blocks,), jnp.float32, least / len(shards), largest / len(shards))
        return jnp.repeat(jnp.exp(heights), shape[position] // blocks).reshape((-1,) + (1,) * (len(shape) - position - 1))

    factor_of = one(*shards[0])
    for cut in shards[1:]:
        factor_of = factor_of * one(*cut)
    return factor_of


def scatter_about(key, shape, scale, bound, shards=(), kind=jnp.bfloat16):
    values = jax.random.normal(key, shape, jnp.float32) * scale
    if len(shards) > 0:
        values = block_levels(key, shape, shards, -0.22, 0.18) * values
    return jnp.clip(values, min=-bound, max=bound).astype(kind)


def setup_inputs(seed: int = 0) -> dict:
    key_list = jax.random.split(jax.random.key(seed), 17)
    return {
        "residual": scatter_about(key_list[0], (SEQ, D), 1.0, 6.0, ((0, 128),)),
        "query_small": draw_query_small(jax.random.fold_in(key_list[16], 71), 0),
        "key_small": draw_key_small(jax.random.fold_in(key_list[16], 71), 0),
        "value_small": scatter_about(key_list[3], (SEQ, HA, VD), 1.0, 6.0, ((0, 16), (1, 8))),
        "query_large": draw_query_large(jax.random.fold_in(key_list[16], 71), 0),
        "key_large": draw_key_large(jax.random.fold_in(key_list[16], 71), 0),
        "value_large": scatter_about(key_list[6], (SEQ, HB, VD), 1.0, 6.0, ((0, 16), (1, 8))),
        "lambda_small": jnp.clip(0.3 + 0.5 * jax.random.uniform(key_list[7], (HA,), jnp.float32) ** block_levels(key_list[7], (HA,), ((0, 8),), -0.2, 0.2), 0.3, 0.8),
        "lambda_large": jnp.clip(0.3 + 0.5 * jax.random.uniform(key_list[8], (HB,), jnp.float32) ** block_levels(key_list[8], (HB,), ((0, 8),), -0.2, 0.2), 0.3, 0.8),
        "head_gain": jnp.clip(1.0 + 0.18 * jax.random.normal(key_list[9], (VD,), jnp.float32), 0.1, 1.9),
        "output_small": scatter_about(key_list[10], (HA * VD, D), ((HA + HB) * VD) ** -0.5, 0.125, ((0, 8),)),
        "output_large": scatter_about(key_list[11], (HB * VD, D), ((HA + HB) * VD) ** -0.5, 0.125, ((0, 8),)),
        "norm_gain": jnp.clip(1.0 + 0.18 * jax.random.normal(key_list[12], (D,), jnp.float32), 0.1, 1.9),
        "gate_weight": scatter_about(key_list[13], (D, FF), D ** -0.5, 0.125, ((0, 16), (1, 8))),
        "up_weight": scatter_about(key_list[14], (D, FF), D ** -0.5, 0.125, ((0, 16), (1, 8))),
        "down_weight": scatter_about(key_list[15], (FF, D), (FF // 16) ** -0.5, 0.3125, ((0, 8), (1, 16))),
    }


residual_scale = 8.0 ** 0.25
branch_scale = 0.8
norm_epsilon = 1e-05
masked_score = -1e+30

def head_group(queries, key_rows, values, lambdas, head_gain):
    length, head_count, doubled = queries.shape
    head_size = doubled // 2
    score_scale = head_size ** (-0.5)
    query_maps = queries.reshape(length, head_count, 2, head_size).astype(jnp.float32)
    key_maps = key_rows.reshape(length, head_count, 2, head_size).astype(jnp.float32)
    value_rows = values.astype(jnp.float32)
    block_size = math.gcd(length, 256)
    key_index = jnp.arange(length, dtype=jnp.int32)

    def one_block(block_index):
        offset = block_index * block_size
        query_block = lax.dynamic_slice_in_dim(query_maps, offset, block_size, 0)
        scores = jnp.einsum('qhmd,khmd->hmqk', query_block, key_maps) * score_scale
        query_index = offset + jnp.arange(block_size, dtype=jnp.int32)
        visible = key_index[None, :] <= query_index[:, None]
        scores = jnp.where(visible, scores, masked_score)
        highest = lax.optimization_barrier(jnp.max(scores, axis=-1, keepdims=True))
        weights = jnp.where(visible, jnp.exp(scores - highest), 0.0)
        totals = lax.optimization_barrier(jnp.sum(weights, axis=-1))
        rounded = lax.optimization_barrier(weights.astype(jnp.bfloat16)).astype(jnp.float32)
        map_out = jnp.einsum('hmqk,khe->hmqe', rounded, value_rows) / totals[..., None]
        combined = map_out[:, 0] - lambdas[:, None, None] * map_out[:, 1]
        mean_square = lax.optimization_barrier(jnp.mean(combined * combined, axis=-1, keepdims=True))
        normed = combined * lax.rsqrt(mean_square + norm_epsilon) * head_gain * branch_scale
        return jnp.transpose(normed, (1, 0, 2)).astype(jnp.bfloat16)
    blocks = lax.map(one_block, jnp.arange(length // block_size, dtype=jnp.int32))
    return blocks.reshape(length, head_count * values.shape[2])

def layer_norm(values, gains):
    centered = values - lax.optimization_barrier(jnp.mean(values, axis=-1, keepdims=True))
    variance = lax.optimization_barrier(jnp.mean(centered * centered, axis=-1, keepdims=True))
    return centered * lax.rsqrt(variance + norm_epsilon) * gains

def reference(residual, query_small, key_small, value_small, query_large, key_large, value_large, lambda_small, lambda_large, head_gain, output_small, output_large, norm_gain, gate_weight, up_weight, down_weight):
    attended_small = head_group(query_small, key_small, value_small, lambda_small, head_gain)
    attended_large = head_group(query_large, key_large, value_large, lambda_large, head_gain)
    mixed_sum = jnp.dot(attended_small, output_small, preferred_element_type=jnp.float32) + jnp.dot(attended_large, output_large, preferred_element_type=jnp.float32)
    pre_norm = residual_scale * residual.astype(jnp.float32) + mixed_sum
    normed = layer_norm(pre_norm, norm_gain).astype(jnp.bfloat16)
    gate_rows = jnp.dot(normed, gate_weight, preferred_element_type=jnp.float32)
    up_rows = jnp.dot(normed, up_weight, preferred_element_type=jnp.float32)
    hidden = (jax.nn.silu(gate_rows) * up_rows).astype(jnp.bfloat16)
    down_sum = jnp.dot(hidden, down_weight, preferred_element_type=jnp.float32)
    return (residual_scale * normed.astype(jnp.float32) + 0.5 * down_sum).astype(jnp.bfloat16)
```

```python
import math

import jax
import jax.numpy as jnp
from jax import lax
from jax.experimental import pallas as pl
from jax.experimental.pallas import tpu as pltpu
from jax.sharding import PartitionSpec as P

residual_scale = 8.0**0.25
branch_scale = 0.8
norm_epsilon = 1e-05
masked_score = -1e30
log2e = math.log2(math.e)
MESH = pl.DeviceIdType.MESH
BF = jnp.bfloat16
F32 = jnp.float32
CH = 512


def remote(src, dst, ssem, rsem, sp, tp):
    return pltpu.make_async_remote_copy(
        src_ref=src, dst_ref=dst, send_sem=ssem, recv_sem=rsem, device_id=(sp, tp), device_id_type=MESH
    )


def attention_kernel(
    qs, ql, ks, kl, vs, vl, lam_in, gain, osm, ola, res, ngain,
    out,
    kv, qb, qz, lam, acc, mx, wo, ob, att, pre,
    q_ssem, q_rsem, x_ssem, kv_rsem, up_ssem, dn_ssem, pr_ssem,
    wu_ssem, wd_ssem, wp_ssem, w_rsem, o_ssem, o_rsem, l_sem,
):
    sp, tp = lax.axis_index("sp"), lax.axis_index("tp")
    z, x, y, c = sp // 4, sp % 4, tp // 2, tp % 2
    kind = x % 2
    large = kind == 1
    zu, zd, z2 = (z + 1) % 4, (z + 3) % 4, (z + 2) % 4
    yu, yd, y2 = (y + 1) % 4, (y + 3) % 4, (y + 2) % 4
    r = 2 * (3 - z) + c
    lo_chunk, hi_chunk = r, 15 - r

    def put(src, dst, ssem, rsem, dsp, dtp):
        same = jnp.logical_and(dsp == sp, dtp == tp)

        @pl.when(same)
        def _():
            pltpu.make_async_copy(src, dst, rsem).start()

        @pl.when(jnp.logical_not(same))
        def _():
            remote(src, dst, ssem, rsem, dsp, dtp).start()

    def put_done(src, dst, ssem, rsem, dsp, dtp):
        same = jnp.logical_and(dsp == sp, dtp == tp)

        @pl.when(jnp.logical_not(same))
        def _():
            remote(src, dst, ssem, rsem, dsp, dtp).wait_send()

    def got(dst, rsem):
        pltpu.make_async_copy(dst, dst, rsem).wait()

    dcore = 2 * y + x % 2
    small_sp, large_sp = 4 * z + 2 * c, 4 * z + 2 * c + 1
    kv_puts = [
        (ks, kv.at[sp, 0], x_ssem.at[0], kv_rsem.at[sp, 0], small_sp, dcore),
        (vs, kv.at[sp, 1], x_ssem.at[1], kv_rsem.at[sp, 1], small_sp, dcore),
        (kl.at[:, pl.ds(0, 128)], kv.at[sp, 0], x_ssem.at[2], kv_rsem.at[sp, 0], large_sp, dcore),
        (vl, kv.at[sp, 1], x_ssem.at[3], kv_rsem.at[sp, 1], large_sp, dcore),
        (kl.at[:, pl.ds(128, 128)], kv.at[sp, 2], x_ssem.at[4], kv_rsem.at[sp, 2], large_sp, dcore),
    ]
    low = jnp.minimum(sp, 15 - sp)
    hi = sp // 8
    qsp = 4 * (3 - low // 2) + 2 * c
    qtp = 2 * y + low % 2
    q_puts = [
        (qs, qb.at[hi, 0], q_ssem.at[0], q_rsem.at[hi, 0], qsp, qtp),
        (ql.at[:, pl.ds(0, 128)], qb.at[hi, 0], q_ssem.at[1], q_rsem.at[hi, 0], qsp + 1, qtp),
        (ql.at[:, pl.ds(128, 128)], qb.at[hi, 1], q_ssem.at[2], q_rsem.at[hi, 1], qsp + 1, qtp),
        (lam_in.at[0], lam.at[hi], q_ssem.at[3], q_rsem.at[hi, 2], qsp, qtp),
        (lam_in.at[1], lam.at[hi], q_ssem.at[4], q_rsem.at[hi, 2], qsp + 1, qtp),
    ]
    for p in kv_puts:
        put(*p)
    for p in q_puts:
        put(*p)

    wu, wd = 2 * yu + c, 2 * yd + c
    partner = 2 * y + 1 - c

    def w_send(slot, ssem, dtp, src=None):
        ref = wo.at[slot]
        return remote(ref if src is None else src, ref, ssem, w_rsem.at[slot], sp, dtp)

    own_a, own_b = tp, 8 + tp
    w_own = [
        w_send(own_a, wu_ssem.at[0], wu, osm), w_send(own_b, wd_ssem.at[0], wd, ola),
        w_send(own_b, wu_ssem.at[1], wu, ola), w_send(own_a, wd_ssem.at[1], wd, osm),
        w_send(own_a, wp_ssem.at[0], partner, osm), w_send(own_b, wp_ssem.at[1], partner, ola),
    ]
    for d in w_own:
        d.start()
    pltpu.make_async_copy(osm, wo.at[own_a], l_sem.at[0]).start()
    pltpu.make_async_copy(ola, wo.at[own_b], l_sem.at[1]).start()
    fwd_a, fwd_b = wd, 8 + wu
    w_f1 = [
        (fwd_a, w_send(fwd_a, wu_ssem.at[2], wu), w_send(fwd_a, wp_ssem.at[2], partner)),
        (fwd_b, w_send(fwd_b, wd_ssem.at[2], wd), w_send(fwd_b, wp_ssem.at[3], partner)),
    ]
    w_f2 = [
        (8 + wd, w_send(8 + wd, wp_ssem.at[4], partner)),
        (wu, w_send(wu, wp_ssem.at[5], partner)),
    ]
    w2 = 2 * y2 + c
    w_f3 = [
        (w2, w_send(w2, wp_ssem.at[6], partner)),
        (8 + w2, w_send(8 + w2, wp_ssem.at[7], partner)),
    ]

    def w_forward(items):
        for item in items:
            got(wo.at[item[0]], w_rsem.at[item[0]])
            for d in item[1:]:
                d.start()

    acc[...] = jnp.zeros_like(acc)
    mx[...] = jnp.full_like(mx, masked_score)

    for h in range(2):
        got(qb.at[h, 0], q_rsem.at[h, 0])
        got(lam.at[h], q_rsem.at[h, 2])

        @pl.when(large)
        def _():
            got(qb.at[h, 1], q_rsem.at[h, 1])
            qz[h, 0] = qb[h, 0]
            qz[h, 1] = qb[h, 1]

        @pl.when(jnp.logical_not(large))
        def _():
            both = qb[h, 0]
            first = lax.broadcasted_iota(jnp.int32, (CH, 128), 1) < 64
            qz[h, 0] = jnp.where(first, both, jnp.zeros_like(both))
            qz[h, 1] = jnp.where(first, jnp.zeros_like(both), both)

    factor = jnp.where(large, log2e * 128**-0.5, log2e * 64**-0.5).astype(F32)
    half = CH // 2

    def absorb(h, j, diagonal):
        values = jnp.concatenate([kv[j, 1], jnp.ones((CH, 128), BF)], axis=1)
        for m in range(2):
            keys = kv[j, 2 * m * kind]
            for t in range(2):
                rows = pl.ds(t * half, half)
                s = lax.dot_general(
                    qz[h, m, rows, :], keys, (((1,), (1,)), ((), ())), preferred_element_type=F32
                )
                if diagonal:
                    qi = lax.broadcasted_iota(jnp.int32, (half, CH), 0) + t * half
                    ki = lax.broadcasted_iota(jnp.int32, (half, CH), 1)
                    s = jnp.where(ki <= qi, s, masked_score)
                old = mx[h, m, rows, :]
                new = jnp.maximum(old, jnp.max(s, axis=1, keepdims=True))
                mx[h, m, rows, :] = new
                p = jnp.exp2((s - new[:, :1]) * factor)
                fade = jnp.exp2((old - new) * factor)
                pv = jnp.dot(p.astype(BF), values, preferred_element_type=F32)
                acc[h, m, rows, 0:128] = acc[h, m, rows, 0:128] * fade + pv[:, 0:128]
                acc[h, m, rows, 128:256] = acc[h, m, rows, 128:256] * fade + pv[:, 128:256]

    def kv_send(j, slab, ssem, dsp, dtp):
        return remote(kv.at[j, slab], kv.at[j, slab], ssem, kv_rsem.at[j, slab], dsp, dtp)

    def slabs(fn):
        fn(0)
        fn(1)

        @pl.when(large)
        def _():
            fn(2)

    def route(i):
        own = i < 2
        off = jnp.where(own, 0, jnp.where((i == 2) | (i == 4), 3, jnp.where(i < 6, 1, 2)))
        part = jnp.where((i == 0) | (i == 2) | (i == 5) | (i == 6), 0, 1)
        level = (z + off) % 4
        up = own | (i == 2)
        down = own | (i == 3)
        return level, part, up, down

    def kv_moves(i, act):
        level, part, up, down = route(i)
        j = 4 * level + 2 * part + c

        def one(s):
            @pl.when(up)
            def _():
                act(kv_send(j, s, up_ssem.at[jnp.minimum(i, 2), s], 4 * zu + x, tp))

            @pl.when(down)
            def _():
                act(kv_send(j, s, dn_ssem.at[jnp.minimum(i, 2), s], 4 * zd + x, tp))

            act(kv_send(j, s, pr_ssem.at[i, s], sp, partner))

        slabs(one)

    def phase(i, carry):
        level, part, up, down = route(i)
        first = 4 * level + 2 * part
        mine, other = first + c, first + 1 - c
        slabs(lambda s: got(kv.at[mine, s], kv_rsem.at[mine, s]))
        kv_moves(i, lambda d: d.start())

        @pl.when(i == 4)
        def _():
            w_forward(w_f1)

        @pl.when(i == 6)
        def _():
            w_forward(w_f2)

        slabs(lambda s: got(kv.at[other, s], kv_rsem.at[other, s]))
        n_lo = jnp.clip(lo_chunk - first + 1, 0, 2)
        n_hi = jnp.clip(hi_chunk - first + 1, 0, 2)

        def step(k, cc):
            h = jnp.where(k >= n_lo, 1, 0)
            j = first + k - h * n_lo
            diagonal = j == jnp.where(h == 1, hi_chunk, lo_chunk)

            @pl.when(diagonal)
            def _():
                absorb(h, j, True)

            @pl.when(jnp.logical_not(diagonal))
            def _():
                absorb(h, j, False)

            return cc

        lax.fori_loop(0, n_lo + n_hi, step, 0)
        return carry

    lax.fori_loop(0, 8, phase, 0)

    slot = 8 * kind + 2 * y + x // 2
    for h in range(2):
        for t in range(2):
            rows = pl.ds(t * half, half)
            one = acc[h, 0, rows, 0:128] / acc[h, 0, rows, 128:256]
            two = acc[h, 1, rows, 0:128] / acc[h, 1, rows, 128:256]
            combined = one - lam[h, 0:1, :] * two
            square = jnp.mean(combined * combined, axis=1, keepdims=True)
            normed = combined * lax.rsqrt(square + norm_epsilon) * gain[...] * branch_scale
            ob[h, rows, :] = normed.astype(BF)
        dsp = hi_chunk if h == 1 else lo_chunk
        for t in range(8):
            put(ob.at[h, pl.ds(64 * t, 64), :], att.at[slot], o_ssem.at[h, t], o_rsem.at[slot], dsp, t)

    w_forward(w_f3)
    pltpu.make_async_copy(osm, wo.at[own_a], l_sem.at[0]).wait()
    pltpu.make_async_copy(ola, wo.at[own_b], l_sem.at[1]).wait()
    for yy in (y, yu, yd, y2):
        for off in (0, 8):
            s = 2 * yy + 1 - c + off
            got(wo.at[s], w_rsem.at[s])
    for s in range(16):
        got(att.at[s], o_rsem.at[s])
    rows = jnp.concatenate([att[s] for s in range(16)], axis=1)

    def project(n, carry):
        cols = pl.ds(pl.multiple_of(n * 512, 512), 512)
        w = wo[:, :, cols].reshape(2048, 512)
        pre[:, cols] = residual_scale * res[:, cols].astype(F32) + jnp.dot(
            rows, w, preferred_element_type=F32
        )
        return carry

    lax.fori_loop(0, 4, project, 0)
    values = pre[...]
    centered = values - jnp.mean(values, axis=1, keepdims=True)
    variance = jnp.mean(centered * centered, axis=1, keepdims=True)
    out[...] = (centered * lax.rsqrt(variance + norm_epsilon) * ngain[...]).astype(BF)

    for p in kv_puts:
        put_done(*p)
    for p in q_puts:
        put_done(*p)
    for d in w_own:
        d.wait_send()
    for item in w_f1 + w_f2 + w_f3:
        for d in item[1:]:
            d.wait_send()

    def drain(i, carry):
        kv_moves(i, lambda d: d.wait_send())
        return carry

    lax.fori_loop(0, 8, drain, 0)
    for h in range(2):
        dsp = hi_chunk if h == 1 else lo_chunk
        for t in range(8):
            put_done(ob.at[h, pl.ds(64 * t, 64), :], att.at[slot], o_ssem.at[h, t], o_rsem.at[slot], dsp, t)


def attention(*args):
    dma = pltpu.SemaphoreType.DMA
    return pl.pallas_call(
        attention_kernel,
        name="attention",
        out_shape=jax.ShapeDtypeStruct((64, 2048), BF),
        in_specs=[pl.BlockSpec(memory_space=pltpu.VMEM)] * len(args),
        out_specs=pl.BlockSpec(memory_space=pltpu.VMEM),
        scratch_shapes=[
            pltpu.VMEM((16, 3, CH, 128), BF),
            pltpu.VMEM((2, 2, CH, 128), BF),
            pltpu.VMEM((2, 2, CH, 128), BF),
            pltpu.VMEM((2, 8, 128), F32),
            pltpu.VMEM((2, 2, CH, 256), F32),
            pltpu.VMEM((2, 2, CH, 128), F32),
            pltpu.VMEM((16, 128, 2048), BF),
            pltpu.VMEM((2, CH, 128), BF),
            pltpu.VMEM((16, 64, 128), BF),
            pltpu.VMEM((64, 2048), F32),
            dma((5,)), dma((2, 3)), dma((5,)), dma((16, 3)), dma((3, 3)), dma((3, 3)), dma((8, 3)),
            dma((3,)), dma((3,)), dma((8,)), dma((16,)), dma((2, 8)), dma((16,)), dma((2,)),
        ],
        compiler_params=pltpu.CompilerParams(has_side_effects=True, vmem_limit_bytes=60 * 1024 * 1024),
        cost_estimate=pl.CostEstimate(flops=8 * 10**9, bytes_accessed=10**8, transcendentals=10**7),
    )(*args)


def rows_first(arrays, axis, dims):
    turned = [jnp.moveaxis(a, dim, 0) for a, dim in zip(arrays, dims)]
    both = jnp.concatenate([t.reshape(len(t), -1) for t in turned], axis=1)
    whole, at, finished = (lax.all_gather(both, axis, axis=0, tiled=True), 0, [])
    for t, dim in zip(turned, dims):
        share = whole[:, at : at + t[0].size].reshape(-1, *t.shape[1:])
        finished.append(jnp.moveaxis(share, 0, dim))
        at += t[0].size
    return tuple(finished)


def split_up(array, dim, devices):
    before, after = (array.shape[:dim], array.shape[dim + 1 :])
    return jnp.moveaxis(array.reshape(*before, devices, -1, *after), dim, 0)


def sent_and_summed(array, axis, dim):
    devices = lax.axis_size(axis)
    tiles = lax.all_to_all(split_up(array, dim, devices), axis, 0, 0, tiled=True)
    return jnp.sum(tiles.astype(jnp.float32), axis=0)


def in_order(tiles, dim):
    dims = list(tiles.shape[1:])
    dims[dim] *= tiles.shape[0]
    return jnp.moveaxis(tiles, 0, dim).reshape(dims)


def from_everyone(array, axis):
    devices = lax.axis_size(axis)
    return lax.all_to_all(jnp.broadcast_to(array[None], (devices, *array.shape)), axis, 0, 0, tiled=True)


def per_device(
    residual, query_small, key_small, value_small, query_large, key_large, value_large,
    lambda_small, lambda_large, head_gain, output_small, output_large, norm_gain,
    gate_weight, up_weight, down_weight,
):
    gate_full, up_full, down_full = rows_first((gate_weight, up_weight, down_weight), "sp", (0, 0, 1))
    flat = lambda a: a.reshape(a.shape[0], a.shape[2])
    lam = jnp.broadcast_to(jnp.stack([lambda_small, lambda_large]).reshape(2, 1, 1), (2, 8, 128))
    normed = attention(
        flat(query_small), flat(query_large), flat(key_small), flat(key_large), flat(value_small),
        flat(value_large), lam, head_gain.reshape(1, 128), output_small, output_large, residual,
        norm_gain.reshape(1, 2048),
    )
    whole_rows = in_order(from_everyone(normed, "tp"), 0)
    gate_rows = jnp.dot(whole_rows, gate_full, preferred_element_type=jnp.float32)
    up_rows = jnp.dot(whole_rows, up_full, preferred_element_type=jnp.float32)
    hidden = (jax.nn.silu(gate_rows) * up_rows).astype(jnp.bfloat16)
    down_sum = sent_and_summed(
        jnp.dot(hidden, down_full, preferred_element_type=jnp.float32).astype(jnp.bfloat16), "tp", 0
    )
    return (residual_scale * normed.astype(jnp.float32) + 0.5 * down_sum).astype(jnp.bfloat16)


def solution(mesh):
    in_specs = (
        P(("sp", "tp"), None),
        P("sp", "tp", None), P("sp", "tp", None), P("sp", "tp", None),
        P("sp", "tp", None), P("sp", "tp", None), P("sp", "tp", None),
        P("tp"), P("tp"), P(), P("tp", None), P("tp", None), P(),
        P("sp", "tp"), P("sp", "tp"), P("tp", "sp"),
    )
    return jax.shard_map(
        per_device, mesh=mesh, in_specs=in_specs, out_specs=P(("sp", "tp"), None), check_vma=False
    )
```

```python
import math

import jax
import jax.numpy as jnp
from jax import lax
from jax.experimental import pallas as pl
from jax.experimental.pallas import tpu as pltpu
from jax.sharding import PartitionSpec as P

residual_scale = 8.0**0.25
branch_scale = 0.8
norm_epsilon = 1e-05
masked_score = -1e30
log2e = math.log2(math.e)
MESH = pl.DeviceIdType.MESH
BF = jnp.bfloat16
F32 = jnp.float32
CH = 512


def remote(src, dst, ssem, rsem, sp, tp):
    return pltpu.make_async_remote_copy(
        src_ref=src, dst_ref=dst, send_sem=ssem, recv_sem=rsem, device_id=(sp, tp), device_id_type=MESH
    )


def block_kernel(
    qs, ql, ks, kl, vs, vl, lam_in, gain, osm, ola, res, ngain, gw, uw, dw,
    out,
    kv, qb, qz, lam, acc, mx, wo, ob, att, pre, wt, nb, psend, precv, mine_f, rsend, rrecv, tbuf,
    q_ssem, q_rsem, x_ssem, kv_rsem, up_ssem, dn_ssem, pr_ssem,
    wu_ssem, wd_ssem, wp_ssem, w_rsem, o_ssem, o_rsem, l_sem,
    g_ssem, g_rsem, nu_ssem, nd_ssem, np_ssem, n_rsem, p_ssem, p_rsem, r_ssem, r_rsem, t_rsem,
):
    sp, tp = lax.axis_index("sp"), lax.axis_index("tp")
    z, x, y, c = sp // 4, sp % 4, tp // 2, tp % 2
    kind = x % 2
    large = kind == 1
    zu, zd, z2 = (z + 1) % 4, (z + 3) % 4, (z + 2) % 4
    yu, yd, y2 = (y + 1) % 4, (y + 3) % 4, (y + 2) % 4
    xu, xd, x2 = (x + 1) % 4, (x + 3) % 4, (x + 2) % 4
    r = 2 * (3 - z) + c
    lo_chunk, hi_chunk = r, 15 - r

    def put(src, dst, ssem, rsem, dsp, dtp):
        same = jnp.logical_and(dsp == sp, dtp == tp)

        @pl.when(same)
        def _():
            pltpu.make_async_copy(src, dst, rsem).start()

        @pl.when(jnp.logical_not(same))
        def _():
            remote(src, dst, ssem, rsem, dsp, dtp).start()

    def put_done(src, dst, ssem, rsem, dsp, dtp):
        same = jnp.logical_and(dsp == sp, dtp == tp)

        @pl.when(jnp.logical_not(same))
        def _():
            remote(src, dst, ssem, rsem, dsp, dtp).wait_send()

    def got(dst, rsem):
        pltpu.make_async_copy(dst, dst, rsem).wait()

    dcore = 2 * y + x % 2
    small_sp, large_sp = 4 * z + 2 * c, 4 * z + 2 * c + 1
    kv_puts = [
        (ks, kv.at[sp, 0], x_ssem.at[0], kv_rsem.at[sp, 0], small_sp, dcore),
        (vs, kv.at[sp, 1], x_ssem.at[1], kv_rsem.at[sp, 1], small_sp, dcore),
        (kl.at[:, pl.ds(0, 128)], kv.at[sp, 0], x_ssem.at[2], kv_rsem.at[sp, 0], large_sp, dcore),
        (vl, kv.at[sp, 1], x_ssem.at[3], kv_rsem.at[sp, 1], large_sp, dcore),
        (kl.at[:, pl.ds(128, 128)], kv.at[sp, 2], x_ssem.at[4], kv_rsem.at[sp, 2], large_sp, dcore),
    ]
    low = jnp.minimum(sp, 15 - sp)
    hi = sp // 8
    qsp = 4 * (3 - low // 2) + 2 * c
    qtp = 2 * y + low % 2
    q_puts = [
        (qs, qb.at[hi, 0], q_ssem.at[0], q_rsem.at[hi, 0], qsp, qtp),
        (ql.at[:, pl.ds(0, 128)], qb.at[hi, 0], q_ssem.at[1], q_rsem.at[hi, 0], qsp + 1, qtp),
        (ql.at[:, pl.ds(128, 128)], qb.at[hi, 1], q_ssem.at[2], q_rsem.at[hi, 1], qsp + 1, qtp),
        (lam_in.at[0], lam.at[hi], q_ssem.at[3], q_rsem.at[hi, 2], qsp, qtp),
        (lam_in.at[1], lam.at[hi], q_ssem.at[4], q_rsem.at[hi, 2], qsp + 1, qtp),
    ]
    for p in kv_puts:
        put(*p)
    for p in q_puts:
        put(*p)

    own_piece = (gw, uw, dw.at[pl.ds(0, 352), :], dw.at[pl.ds(352, 352), :])

    def piece(s, k):
        return wt.at[s, k] if k < 2 else wt.at[s, 2, pl.ds(352 * (k - 2), 352), :]

    class Ring:
        def __init__(self, at, along_x, first, line):
            self.at, self.first = at, first
            if along_x:
                self.slots = [4 * line + p for p in (x, xd, xu, x2)]
                self.up, self.down = 4 * z + xu, 4 * z + xd
            else:
                self.slots = [4 * p + line for p in (z, zd, zu, z2)]
                self.up, self.down = 4 * zu + x, 4 * zd + x

        def send(self, n, which, k, to, src=None):
            s = self.slots[which]
            ref = piece(s, k)
            return remote(ref if src is None else src, ref, g_ssem.at[self.at, n], g_rsem.at[s, k], to, tp)

        def own_sends(self, from_input=False):
            a, b = self.first, self.first + 1
            sa, sb = (own_piece[a], own_piece[b]) if from_input else (None, None)
            return [
                self.send(0, 0, a, self.up, sa), self.send(1, 0, b, self.down, sb),
                self.send(2, 0, b, self.up, sb), self.send(3, 0, a, self.down, sa),
            ]

        def far_sends(self):
            return self.send(4, 1, self.first, self.up), self.send(5, 2, self.first + 1, self.down)

        def got(self, which, k):
            got(piece(self.slots[which], k), g_rsem.at[self.slots[which], k])

        def own(self, from_input=False):
            for d in self.own_sends(from_input):
                d.start()

        def forward(self):
            f1, f2 = self.far_sends()
            self.got(1, self.first)
            f1.start()
            self.got(2, self.first + 1)
            f2.start()

        def near(self):
            self.got(1, self.first + 1)
            self.got(2, self.first)

        def far(self):
            self.got(3, self.first)
            self.got(3, self.first + 1)

        def drain(self):
            for d in (*self.own_sends(), *self.far_sends()):
                d.wait_send()

    r0 = Ring(0, False, 0, x)
    r1, r2, r3, r4 = [Ring(1 + n, True, 0, line) for n, line in enumerate((z, zd, zu, z2))]
    r5 = Ring(5, True, 2, z)
    r6, r7, r8, r9 = [Ring(6 + n, False, 2, line) for n, line in enumerate((x, xd, xu, x2))]
    for ring in (r0, r1, r5, r6):
        ring.own(True)

    wu, wd = 2 * yu + c, 2 * yd + c
    partner = 2 * y + 1 - c

    def w_send(slot, ssem, dtp, src=None):
        ref = wo.at[slot]
        return remote(ref if src is None else src, ref, ssem, w_rsem.at[slot], sp, dtp)

    own_a, own_b = tp, 8 + tp
    w_own = [
        w_send(own_a, wu_ssem.at[0], wu, osm), w_send(own_b, wd_ssem.at[0], wd, ola),
        w_send(own_b, wu_ssem.at[1], wu, ola), w_send(own_a, wd_ssem.at[1], wd, osm),
        w_send(own_a, wp_ssem.at[0], partner, osm), w_send(own_b, wp_ssem.at[1], partner, ola),
    ]
    for d in w_own:
        d.start()
    pltpu.make_async_copy(osm, wo.at[own_a], l_sem.at[0]).start()
    pltpu.make_async_copy(ola, wo.at[own_b], l_sem.at[1]).start()
    fwd_a, fwd_b = wd, 8 + wu
    w_f1 = [
        (fwd_a, w_send(fwd_a, wu_ssem.at[2], wu), w_send(fwd_a, wp_ssem.at[2], partner)),
        (fwd_b, w_send(fwd_b, wd_ssem.at[2], wd), w_send(fwd_b, wp_ssem.at[3], partner)),
    ]
    w_f2 = [
        (8 + wd, w_send(8 + wd, wp_ssem.at[4], partner)),
        (wu, w_send(wu, wp_ssem.at[5], partner)),
    ]
    w2 = 2 * y2 + c
    w_f3 = [
        (w2, w_send(w2, wp_ssem.at[6], partner)),
        (8 + w2, w_send(8 + w2, wp_ssem.at[7], partner)),
    ]

    def w_forward(items):
        for item in items:
            got(wo.at[item[0]], w_rsem.at[item[0]])
            for d in item[1:]:
                d.start()

    acc[...] = jnp.zeros_like(acc)
    mx[...] = jnp.full_like(mx, masked_score)

    for h in range(2):
        got(qb.at[h, 0], q_rsem.at[h, 0])
        got(lam.at[h], q_rsem.at[h, 2])

        @pl.when(large)
        def _():
            got(qb.at[h, 1], q_rsem.at[h, 1])
            qz[h, 0] = qb[h, 0]
            qz[h, 1] = qb[h, 1]

        @pl.when(jnp.logical_not(large))
        def _():
            both = qb[h, 0]
            first = lax.broadcasted_iota(jnp.int32, (CH, 128), 1) < 64
            qz[h, 0] = jnp.where(first, both, jnp.zeros_like(both))
            qz[h, 1] = jnp.where(first, jnp.zeros_like(both), both)

    factor = jnp.where(large, log2e * 128**-0.5, log2e * 64**-0.5).astype(F32)
    half = CH // 2

    def absorb(h, j, diagonal):
        values = jnp.concatenate([kv[j, 1], jnp.ones((CH, 128), BF)], axis=1)
        for m in range(2):
            keys = kv[j, 2 * m * kind]
            for t in range(2):
                rows = pl.ds(t * half, half)
                s = lax.dot_general(
                    qz[h, m, rows, :], keys, (((1,), (1,)), ((), ())), preferred_element_type=F32
                )
                if diagonal:
                    qi = lax.broadcasted_iota(jnp.int32, (half, CH), 0) + t * half
                    ki = lax.broadcasted_iota(jnp.int32, (half, CH), 1)
                    s = jnp.where(ki <= qi, s, masked_score)
                old = mx[h, m, rows, :]
                new = jnp.maximum(old, jnp.max(s, axis=1, keepdims=True))
                mx[h, m, rows, :] = new
                p = jnp.exp2((s - new[:, :1]) * factor)
                fade = jnp.exp2((old - new) * factor)
                pv = jnp.dot(p.astype(BF), values, preferred_element_type=F32)
                acc[h, m, rows, 0:128] = acc[h, m, rows, 0:128] * fade + pv[:, 0:128]
                acc[h, m, rows, 128:256] = acc[h, m, rows, 128:256] * fade + pv[:, 128:256]

    def kv_send(j, slab, ssem, dsp, dtp):
        return remote(kv.at[j, slab], kv.at[j, slab], ssem, kv_rsem.at[j, slab], dsp, dtp)

    def slabs(fn):
        fn(0)
        fn(1)

        @pl.when(large)
        def _():
            fn(2)

    def route(i):
        own = i < 2
        off = jnp.where(own, 0, jnp.where((i == 2) | (i == 4), 3, jnp.where(i < 6, 1, 2)))
        part = jnp.where((i == 0) | (i == 2) | (i == 5) | (i == 6), 0, 1)
        level = (z + off) % 4
        up = own | (i == 2)
        down = own | (i == 3)
        return level, part, up, down

    def kv_moves(i, act):
        level, part, up, down = route(i)
        j = 4 * level + 2 * part + c

        def one(s):
            @pl.when(up)
            def _():
                act(kv_send(j, s, up_ssem.at[jnp.minimum(i, 2), s], 4 * zu + x, tp))

            @pl.when(down)
            def _():
                act(kv_send(j, s, dn_ssem.at[jnp.minimum(i, 2), s], 4 * zd + x, tp))

            act(kv_send(j, s, pr_ssem.at[i, s], sp, partner))

        slabs(one)

    def phase(i, carry):
        level, part, up, down = route(i)
        first = 4 * level + 2 * part
        mine, other = first + c, first + 1 - c

        @pl.when(i == 2)
        def _():
            r0.forward()
            r0.near()
            r2.own()
            r3.own()

        @pl.when(i == 4)
        def _():
            r1.forward()
            r5.forward()
            r5.near()
            r7.own()
            r8.own()

        @pl.when(i == 6)
        def _():
            r0.far()
            r4.own()
            r5.far()
            r9.own()

        slabs(lambda s: got(kv.at[mine, s], kv_rsem.at[mine, s]))
        kv_moves(i, lambda d: d.start())

        @pl.when(i == 4)
        def _():
            w_forward(w_f1)

        @pl.when(i == 6)
        def _():
            w_forward(w_f2)

        slabs(lambda s: got(kv.at[other, s], kv_rsem.at[other, s]))
        n_lo = jnp.clip(lo_chunk - first + 1, 0, 2)
        n_hi = jnp.clip(hi_chunk - first + 1, 0, 2)

        def step(k, cc):
            h = jnp.where(k >= n_lo, 1, 0)
            j = first + k - h * n_lo
            diagonal = j == jnp.where(h == 1, hi_chunk, lo_chunk)

            @pl.when(diagonal)
            def _():
                absorb(h, j, True)

            @pl.when(jnp.logical_not(diagonal))
            def _():
                absorb(h, j, False)

            return cc

        lax.fori_loop(0, n_lo + n_hi, step, 0)
        return carry

    lax.fori_loop(0, 8, phase, 0)

    slot = 8 * kind + 2 * y + x // 2
    for h in range(2):
        for t in range(2):
            rows = pl.ds(t * half, half)
            one = acc[h, 0, rows, 0:128] / acc[h, 0, rows, 128:256]
            two = acc[h, 1, rows, 0:128] / acc[h, 1, rows, 128:256]
            combined = one - lam[h, 0:1, :] * two
            square = jnp.mean(combined * combined, axis=1, keepdims=True)
            normed = combined * lax.rsqrt(square + norm_epsilon) * gain[...] * branch_scale
            ob[h, rows, :] = normed.astype(BF)
        dsp = hi_chunk if h == 1 else lo_chunk
        for t in range(8):
            put(ob.at[h, pl.ds(64 * t, 64), :], att.at[slot], o_ssem.at[h, t], o_rsem.at[slot], dsp, t)

    r2.forward()
    r3.forward()
    r6.forward()
    r7.forward()
    r8.forward()
    w_forward(w_f3)
    pltpu.make_async_copy(osm, wo.at[own_a], l_sem.at[0]).wait()
    pltpu.make_async_copy(ola, wo.at[own_b], l_sem.at[1]).wait()
    for yy in (y, yu, yd, y2):
        for off in (0, 8):
            s = 2 * yy + 1 - c + off
            got(wo.at[s], w_rsem.at[s])
    for s in range(16):
        got(att.at[s], o_rsem.at[s])
    rows = jnp.concatenate([att[s] for s in range(16)], axis=1)

    def project(n, carry):
        cols = pl.ds(pl.multiple_of(n * 512, 512), 512)
        w = wo[:, :, cols].reshape(2048, 512)
        pre[:, cols] = residual_scale * res[:, cols].astype(F32) + jnp.dot(
            rows, w, preferred_element_type=F32
        )
        return carry

    lax.fori_loop(0, 4, project, 0)
    values = pre[...]
    centered = values - jnp.mean(values, axis=1, keepdims=True)
    variance = jnp.mean(centered * centered, axis=1, keepdims=True)
    normed = (centered * lax.rsqrt(variance + norm_epsilon) * ngain[...]).astype(BF)
    nb[tp, 0] = normed[:, 0:1024]
    nb[tp, 1] = normed[:, 1024:2048]

    def n_send(t, k, ssem, dtp):
        return remote(nb.at[t, k], nb.at[t, k], ssem, n_rsem.at[t, k], sp, dtp)

    n_own = [
        n_send(tp, 0, nu_ssem.at[0], wu), n_send(tp, 1, nd_ssem.at[0], wd),
        n_send(tp, 1, nu_ssem.at[1], wu), n_send(tp, 0, nd_ssem.at[1], wd),
        n_send(tp, 0, np_ssem.at[0], partner), n_send(tp, 1, np_ssem.at[1], partner),
    ]
    n_fwd = [
        (wd, 0, [n_send(wd, 0, nu_ssem.at[2], wu), n_send(wd, 0, np_ssem.at[2], partner)]),
        (wu, 1, [n_send(wu, 1, nd_ssem.at[2], wd), n_send(wu, 1, np_ssem.at[3], partner)]),
        (wd, 1, [n_send(wd, 1, np_ssem.at[4], partner)]),
        (wu, 0, [n_send(wu, 0, np_ssem.at[5], partner)]),
        (w2, 0, [n_send(w2, 0, np_ssem.at[6], partner)]),
        (w2, 1, [n_send(w2, 1, np_ssem.at[7], partner)]),
    ]
    for d in n_own:
        d.start()
    r4.forward()
    r9.forward()
    for t, k, sends in n_fwd:
        got(nb.at[t, k], n_rsem.at[t, k])
        for d in sends:
            d.start()
    wt[sp, 0] = gw[...]
    wt[sp, 1] = uw[...]
    wt[sp, 2] = dw[...]
    for ring in (r1, r2, r3, r4, r6, r7, r8, r9):
        ring.near()
        ring.far()

    def mixer(groups):
        rows = []
        for g, yy in groups:
            t = 2 * yy + 1 - c
            got(nb.at[t, 0], n_rsem.at[t, 0])
            got(nb.at[t, 1], n_rsem.at[t, 1])
            for t in (2 * yy + 1 - c, 2 * yy + c):
                rows.append(jnp.concatenate([nb[t, 0], nb[t, 1]], axis=1))
        rows = jnp.concatenate(rows, axis=0)
        nt = (((1,), (1,)), ((), ()))
        gate = lax.dot_general(
            rows, jnp.concatenate([wt[s, 0] for s in range(16)], axis=1), nt, preferred_element_type=F32
        )
        up = lax.dot_general(
            rows, jnp.concatenate([wt[s, 1] for s in range(16)], axis=1), nt, preferred_element_type=F32
        )
        hidden = (gate / (1.0 + jnp.exp(-gate)) * up).astype(BF)
        for n in range(8):
            cols = pl.ds(256 * n, 256)
            w = jnp.concatenate([wt[2 * n, 2], wt[2 * n + 1, 2]], axis=1)
            part = jnp.dot(hidden, w, preferred_element_type=F32)
            for at, (g, yy) in enumerate(groups):
                psend[g, :, cols] = part[128 * at : 128 * at + 64].astype(BF)
                mine_f[g, :, cols] = part[128 * at + 64 : 128 * at + 128]
        for g, yy in groups:
            p_move(g).start()

    def p_move(g):
        return remote(psend.at[g], precv.at[g], p_ssem.at[g], p_rsem.at[g], sp, partner)

    def pair_sum(g):
        got(precv.at[g], p_rsem.at[g])
        both = (mine_f[g] + precv[g].astype(F32)).astype(BF)
        rsend[g, 0] = both[:, 0:1024]
        rsend[g, 1] = both[:, 1024:2048]

    r_up = remote(rsend.at[1], rrecv.at[0], r_ssem.at[0], r_rsem.at[0], sp, wu)
    r_down = remote(rsend.at[2], rrecv.at[1], r_ssem.at[1], r_rsem.at[1], sp, wd)
    r_a = remote(rsend.at[0, 0], tbuf.at[0], r_ssem.at[2], t_rsem.at[0], sp, wu)
    r_b = remote(rsend.at[0, 1], tbuf.at[1], r_ssem.at[3], t_rsem.at[1], sp, wd)
    f_a = remote(tbuf.at[0], rrecv.at[2, 0], r_ssem.at[4], r_rsem.at[2], sp, wu)
    f_b = remote(tbuf.at[1], rrecv.at[2, 1], r_ssem.at[5], r_rsem.at[3], sp, wd)
    mixer([(0, y2)])
    pair_sum(0)
    r_a.start()
    r_b.start()
    mixer([(1, yu), (2, yd)])
    got(tbuf.at[0], t_rsem.at[0])
    f_a.start()
    got(tbuf.at[1], t_rsem.at[1])
    f_b.start()
    pair_sum(1)
    r_up.start()
    pair_sum(2)
    r_down.start()
    mixer_own = [(3, y)]
    mixer(mixer_own)
    got(precv.at[3], p_rsem.at[3])
    pre[...] = residual_scale * normed.astype(F32) + 0.5 * (mine_f[3] + precv[3].astype(F32))
    got(rrecv.at[0], r_rsem.at[0])
    got(rrecv.at[1], r_rsem.at[1])
    got(rrecv.at[2, 0], r_rsem.at[2])
    got(rrecv.at[2, 1], r_rsem.at[3])
    for k in range(2):
        cols = pl.ds(1024 * k, 1024)
        more = rrecv[0, k].astype(F32) + rrecv[1, k].astype(F32) + rrecv[2, k].astype(F32)
        out[:, cols] = (pre[:, cols] + 0.5 * more).astype(BF)

    for p in kv_puts:
        put_done(*p)
    for p in q_puts:
        put_done(*p)
    for d in w_own:
        d.wait_send()
    for item in w_f1 + w_f2 + w_f3:
        for d in item[1:]:
            d.wait_send()

    for ring in (r0, r1, r2, r3, r4, r5, r6, r7, r8, r9):
        ring.drain()
    for d in n_own:
        d.wait_send()
    for t, k, sends in n_fwd:
        for d in sends:
            d.wait_send()
    for g in range(4):
        p_move(g).wait_send()
    for d in (r_up, r_down, r_a, r_b, f_a, f_b):
        d.wait_send()

    def drain(i, carry):
        kv_moves(i, lambda d: d.wait_send())
        return carry

    lax.fori_loop(0, 8, drain, 0)
    for h in range(2):
        dsp = hi_chunk if h == 1 else lo_chunk
        for t in range(8):
            put_done(ob.at[h, pl.ds(64 * t, 64), :], att.at[slot], o_ssem.at[h, t], o_rsem.at[slot], dsp, t)


def block(*args):
    dma = pltpu.SemaphoreType.DMA
    return pl.pallas_call(
        block_kernel,
        name="block",
        out_shape=jax.ShapeDtypeStruct((64, 2048), BF),
        in_specs=[pl.BlockSpec(memory_space=pltpu.VMEM)] * len(args),
        out_specs=pl.BlockSpec(memory_space=pltpu.VMEM),
        scratch_shapes=[
            pltpu.VMEM((16, 3, CH, 128), BF),
            pltpu.VMEM((2, 2, CH, 128), BF),
            pltpu.VMEM((2, 2, CH, 128), BF),
            pltpu.VMEM((2, 8, 128), F32),
            pltpu.VMEM((2, 2, CH, 256), F32),
            pltpu.VMEM((2, 2, CH, 128), F32),
            pltpu.VMEM((16, 128, 2048), BF),
            pltpu.VMEM((2, CH, 128), BF),
            pltpu.VMEM((16, 64, 128), BF),
            pltpu.VMEM((64, 2048), F32),
            pltpu.VMEM((16, 3, 704, 128), BF),
            pltpu.VMEM((8, 2, 64, 1024), BF),
            pltpu.VMEM((4, 64, 2048), BF),
            pltpu.VMEM((4, 64, 2048), BF),
            pltpu.VMEM((4, 64, 2048), F32),
            pltpu.VMEM((3, 2, 64, 1024), BF),
            pltpu.VMEM((3, 2, 64, 1024), BF),
            pltpu.VMEM((2, 64, 1024), BF),
            dma((5,)), dma((2, 3)), dma((5,)), dma((16, 3)), dma((3, 3)), dma((3, 3)), dma((8, 3)),
            dma((3,)), dma((3,)), dma((8,)), dma((16,)), dma((2, 8)), dma((16,)), dma((2,)),
            dma((10, 6)), dma((16, 4)), dma((3,)), dma((3,)), dma((8,)), dma((8, 2)),
            dma((4,)), dma((4,)), dma((6,)), dma((4,)), dma((2,)),
        ],
        compiler_params=pltpu.CompilerParams(has_side_effects=True, vmem_limit_bytes=60 * 1024 * 1024),
        cost_estimate=pl.CostEstimate(flops=8 * 10**9, bytes_accessed=10**8, transcendentals=10**7),
    )(*args)


def per_device(
    residual, query_small, key_small, value_small, query_large, key_large, value_large,
    lambda_small, lambda_large, head_gain, output_small, output_large, norm_gain,
    gate_weight, up_weight, down_weight,
):
    flat = lambda a: a.reshape(a.shape[0], a.shape[2])
    lam = jnp.broadcast_to(jnp.stack([lambda_small, lambda_large]).reshape(2, 1, 1), (2, 8, 128))
    return block(
        flat(query_small), flat(query_large), flat(key_small), flat(key_large), flat(value_small),
        flat(value_large), lam, head_gain.reshape(1, 128), output_small, output_large, residual,
        norm_gain.reshape(1, 2048), gate_weight.T, up_weight.T, down_weight,
    )


def solution(mesh):
    in_specs = (
        P(("sp", "tp"), None),
        P("sp", "tp", None), P("sp", "tp", None), P("sp", "tp", None),
        P("sp", "tp", None), P("sp", "tp", None), P("sp", "tp", None),
        P("tp"), P("tp"), P(), P("tp", None), P("tp", None), P(),
        P("sp", "tp"), P("sp", "tp"), P("tp", "sp"),
    )
    return jax.shard_map(
        per_device, mesh=mesh, in_specs=in_specs, out_specs=P(("sp", "tp"), None), check_vma=False
    )
```

```python
import math

import jax
import jax.numpy as jnp
from jax import lax
from jax.experimental import pallas as pl
from jax.experimental.pallas import tpu as pltpu
from jax.sharding import PartitionSpec as P

residual_scale = 8.0**0.25
branch_scale = 0.8
norm_epsilon = 1e-05
masked_score = -1e30
log2e = math.log2(math.e)
MESH = pl.DeviceIdType.MESH
BF = jnp.bfloat16
F32 = jnp.float32
CH = 512


def remote(src, dst, ssem, rsem, sp, tp):
    return pltpu.make_async_remote_copy(
        src_ref=src, dst_ref=dst, send_sem=ssem, recv_sem=rsem, device_id=(sp, tp), device_id_type=MESH
    )


def block_kernel(
    qs_in, ql_in, ks_in, kl_in, vs_in, vl_in, lam_in, gain, osm, ola, res, ngain, gw, uw, dw,
    out,
    qs, ql, ks, kl, vs, vl, kv, qb, qz, lam, acc, mx, wo, ob, att, pre, wt, nb, psend, precv, mine_f, rsend, rrecv, tbuf,
    q_ssem, q_rsem, x_ssem, kv_rsem, up_ssem, dn_ssem, pr_ssem,
    wu_ssem, wd_ssem, wp_ssem, w_rsem, o_ssem, o_rsem, l_sem,
    g_ssem, g_rsem, nu_ssem, nd_ssem, np_ssem, n_rsem, p_ssem, p_rsem, r_ssem, r_rsem, t_rsem, i_sem,
):
    sp, tp = lax.axis_index("sp"), lax.axis_index("tp")
    z, x, y, c = sp // 4, sp % 4, tp // 2, tp % 2
    kind = x % 2
    large = kind == 1
    zu, zd, z2 = (z + 1) % 4, (z + 3) % 4, (z + 2) % 4
    yu, yd, y2 = (y + 1) % 4, (y + 3) % 4, (y + 2) % 4
    xu, xd, x2 = (x + 1) % 4, (x + 3) % 4, (x + 2) % 4
    r = 2 * (3 - z) + c
    lo_chunk, hi_chunk = r, 15 - r

    def put(src, dst, ssem, rsem, dsp, dtp):
        same = jnp.logical_and(dsp == sp, dtp == tp)

        @pl.when(same)
        def _():
            pltpu.make_async_copy(src, dst, rsem).start()

        @pl.when(jnp.logical_not(same))
        def _():
            remote(src, dst, ssem, rsem, dsp, dtp).start()

    def put_done(src, dst, ssem, rsem, dsp, dtp):
        same = jnp.logical_and(dsp == sp, dtp == tp)

        @pl.when(jnp.logical_not(same))
        def _():
            remote(src, dst, ssem, rsem, dsp, dtp).wait_send()

    def got(dst, rsem):
        pltpu.make_async_copy(dst, dst, rsem).wait()

    staged = [
        pltpu.make_async_copy(a, b, i_sem.at[n])
        for n, (a, b) in enumerate(
            ((ks_in, ks), (vs_in, vs), (kl_in, kl), (vl_in, vl), (qs_in, qs), (ql_in, ql))
        )
    ]
    for d in staged:
        d.start()
    dcore = 2 * y + x % 2
    small_sp, large_sp = 4 * z + 2 * c, 4 * z + 2 * c + 1
    kv_puts = [
        (ks, kv.at[sp, 0], x_ssem.at[0], kv_rsem.at[sp, 0], small_sp, dcore),
        (vs, kv.at[sp, 1], x_ssem.at[1], kv_rsem.at[sp, 1], small_sp, dcore),
        (kl.at[:, pl.ds(0, 128)], kv.at[sp, 0], x_ssem.at[2], kv_rsem.at[sp, 0], large_sp, dcore),
        (vl, kv.at[sp, 1], x_ssem.at[3], kv_rsem.at[sp, 1], large_sp, dcore),
        (kl.at[:, pl.ds(128, 128)], kv.at[sp, 2], x_ssem.at[4], kv_rsem.at[sp, 2], large_sp, dcore),
    ]
    low = jnp.minimum(sp, 15 - sp)
    hi = sp // 8
    qsp = 4 * (3 - low // 2) + 2 * c
    qtp = 2 * y + low % 2
    q_puts = [
        (qs, qb.at[hi, 0], q_ssem.at[0], q_rsem.at[hi, 0], qsp, qtp),
        (ql.at[:, pl.ds(0, 128)], qb.at[hi, 0], q_ssem.at[1], q_rsem.at[hi, 0], qsp + 1, qtp),
        (ql.at[:, pl.ds(128, 128)], qb.at[hi, 1], q_ssem.at[2], q_rsem.at[hi, 1], qsp + 1, qtp),
        (lam_in.at[0], lam.at[hi], q_ssem.at[3], q_rsem.at[hi, 2], qsp, qtp),
        (lam_in.at[1], lam.at[hi], q_ssem.at[4], q_rsem.at[hi, 2], qsp + 1, qtp),
    ]
    barrier = pltpu.get_barrier_semaphore()

    def greet(dsp, dtp):
        @pl.when(jnp.logical_not(jnp.logical_and(dsp == sp, dtp == tp)))
        def _():
            pl.semaphore_signal(barrier, inc=1, device_id=(dsp, dtp), device_id_type=MESH)

    sources = [(4 * z + c, 2 * y + x // 2), (4 * z + c + 2, 2 * y + x // 2)]
    targets = [(small_sp, dcore), (large_sp, dcore)]
    sources += [(lo_chunk, 2 * y + x // 2), (hi_chunk, 2 * y + x // 2)]
    targets += [(qsp, qtp), (qsp + 1, qtp)]
    near = [(4 * zu + x, tp), (4 * zd + x, tp), (4 * z + xu, tp), (4 * z + xd, tp)]
    near += [(sp, 2 * yu + c), (sp, 2 * yd + c), (sp, 2 * y + 1 - c)]
    sources += near + [(4 * (3 - low // 2) + a, 2 * b + low % 2) for a in range(4) for b in range(4)]
    targets += near + [(a, t) for a in (lo_chunk, hi_chunk) for t in range(8)]
    for d in sources:
        greet(*d)
    count = len(targets)
    for d in targets:
        count -= jnp.logical_and(d[0] == sp, d[1] == tp).astype(jnp.int32)
    with jax.named_scope("barrier"):
        pl.semaphore_wait(barrier, count)
    for d, p in zip(staged, (kv_puts[:1], kv_puts[1:2], kv_puts[2:3] + kv_puts[4:], kv_puts[3:4])):
        d.wait()
        for one in p:
            put(*one)
    for d in staged[4:]:
        d.wait()
    for p in q_puts:
        put(*p)

    own_piece = (gw, uw, dw.at[pl.ds(0, 352), :], dw.at[pl.ds(352, 352), :])

    def piece(s, k):
        return wt.at[s, k] if k < 2 else wt.at[s, 2, pl.ds(352 * (k - 2), 352), :]

    class Ring:
        def __init__(self, at, along_x, first, line):
            self.at, self.first = at, first
            if along_x:
                self.slots = [4 * line + p for p in (x, xd, xu, x2)]
                self.up, self.down = 4 * z + xu, 4 * z + xd
            else:
                self.slots = [4 * p + line for p in (z, zd, zu, z2)]
                self.up, self.down = 4 * zu + x, 4 * zd + x

        def send(self, n, which, k, to, src=None):
            s = self.slots[which]
            ref = piece(s, k)
            return remote(ref if src is None else src, ref, g_ssem.at[self.at, n], g_rsem.at[s, k], to, tp)

        def own_sends(self, from_input=False):
            a, b = self.first, self.first + 1
            sa, sb = (own_piece[a], own_piece[b]) if from_input else (None, None)
            return [
                self.send(0, 0, a, self.up, sa), self.send(1, 0, b, self.down, sb),
                self.send(2, 0, b, self.up, sb), self.send(3, 0, a, self.down, sa),
            ]

        def far_sends(self):
            return self.send(4, 1, self.first, self.up), self.send(5, 2, self.first + 1, self.down)

        def got(self, which, k):
            got(piece(self.slots[which], k), g_rsem.at[self.slots[which], k])

        def own(self, from_input=False):
            for d in self.own_sends(from_input):
                d.start()

        def forward(self):
            f1, f2 = self.far_sends()
            self.got(1, self.first)
            f1.start()
            self.got(2, self.first + 1)
            f2.start()

        def near(self):
            self.got(1, self.first + 1)
            self.got(2, self.first)

        def far(self):
            self.got(3, self.first)
            self.got(3, self.first + 1)

        def drain(self):
            for d in (*self.own_sends(), *self.far_sends()):
                d.wait_send()

    r0 = Ring(0, False, 0, x)
    r1, r2, r3, r4 = [Ring(1 + n, True, 0, line) for n, line in enumerate((z, zd, zu, z2))]
    r5 = Ring(5, True, 2, z)
    r6, r7, r8, r9 = [Ring(6 + n, False, 2, line) for n, line in enumerate((x, xd, xu, x2))]
    for ring in (r0, r1, r5):
        ring.own(True)

    wu, wd = 2 * yu + c, 2 * yd + c
    partner = 2 * y + 1 - c

    def w_send(slot, ssem, dtp, src=None):
        ref = wo.at[slot]
        return remote(ref if src is None else src, ref, ssem, w_rsem.at[slot], sp, dtp)

    own_a, own_b = tp, 8 + tp
    w_own = [
        w_send(own_a, wu_ssem.at[0], wu, osm), w_send(own_b, wd_ssem.at[0], wd, ola),
        w_send(own_b, wu_ssem.at[1], wu, ola), w_send(own_a, wd_ssem.at[1], wd, osm),
        w_send(own_a, wp_ssem.at[0], partner, osm), w_send(own_b, wp_ssem.at[1], partner, ola),
    ]
    for d in w_own:
        d.start()
    pltpu.make_async_copy(osm, wo.at[own_a], l_sem.at[0]).start()
    pltpu.make_async_copy(ola, wo.at[own_b], l_sem.at[1]).start()
    fwd_a, fwd_b = wd, 8 + wu
    w_f1 = [
        (fwd_a, w_send(fwd_a, wu_ssem.at[2], wu), w_send(fwd_a, wp_ssem.at[2], partner)),
        (fwd_b, w_send(fwd_b, wd_ssem.at[2], wd), w_send(fwd_b, wp_ssem.at[3], partner)),
    ]
    w_f2 = [
        (8 + wd, w_send(8 + wd, wp_ssem.at[4], partner)),
        (wu, w_send(wu, wp_ssem.at[5], partner)),
    ]
    w2 = 2 * y2 + c
    w_f3 = [
        (w2, w_send(w2, wp_ssem.at[6], partner)),
        (8 + w2, w_send(8 + w2, wp_ssem.at[7], partner)),
    ]

    def w_forward(items):
        for item in items:
            got(wo.at[item[0]], w_rsem.at[item[0]])
            for d in item[1:]:
                d.start()

    for n, a in enumerate((gw, uw, dw)):
        pltpu.make_async_copy(a, wt.at[sp, n], i_sem.at[6 + n]).start()
    acc[...] = jnp.zeros_like(acc)
    mx[...] = jnp.full_like(mx, masked_score)

    factor = jnp.where(large, log2e * 128**-0.5, log2e * 64**-0.5).astype(F32)
    half = CH // 2

    def absorb(h, j, diagonal):
        values = jnp.concatenate([kv[j, 1], jnp.ones((CH, 128), BF)], axis=1)
        for m in range(2):
            keys = kv[j, 2 * m * kind]
            for t in range(2):
                rows = pl.ds(t * half, half)
                s = lax.dot_general(
                    qz[h, m, rows, :], keys, (((1,), (1,)), ((), ())), preferred_element_type=F32
                )
                if diagonal:
                    qi = lax.broadcasted_iota(jnp.int32, (half, CH), 0) + t * half
                    ki = lax.broadcasted_iota(jnp.int32, (half, CH), 1)
                    s = jnp.where(ki <= qi, s, masked_score)
                old = mx[h, m, rows, :]
                new = jnp.maximum(old, jnp.max(s, axis=1, keepdims=True))
                mx[h, m, rows, :] = new
                p = jnp.exp2((s - new[:, :1]) * factor)
                fade = jnp.exp2((old - new) * factor)
                pv = jnp.dot(p.astype(BF), values, preferred_element_type=F32)
                acc[h, m, rows, 0:128] = acc[h, m, rows, 0:128] * fade + pv[:, 0:128]
                acc[h, m, rows, 128:256] = acc[h, m, rows, 128:256] * fade + pv[:, 128:256]

    def kv_send(j, slab, ssem, dsp, dtp):
        return remote(kv.at[j, slab], kv.at[j, slab], ssem, kv_rsem.at[j, slab], dsp, dtp)

    def slabs(fn):
        fn(0)
        fn(1)

        @pl.when(large)
        def _():
            fn(2)

    def route(i):
        own = i < 2
        off = jnp.where(own, 0, jnp.where((i == 2) | (i == 4), 3, jnp.where(i < 6, 1, 2)))
        part = jnp.where((i == 0) | (i == 2) | (i == 5) | (i == 6), 0, 1)
        level = (z + off) % 4
        up = own | (i == 2)
        down = own | (i == 3)
        return level, part, up, down

    def kv_moves(i, act):
        level, part, up, down = route(i)
        j = 4 * level + 2 * part + c

        def one(s):
            @pl.when(up)
            def _():
                act(kv_send(j, s, up_ssem.at[jnp.minimum(i, 2), s], 4 * zu + x, tp))

            @pl.when(down)
            def _():
                act(kv_send(j, s, dn_ssem.at[jnp.minimum(i, 2), s], 4 * zd + x, tp))

            act(kv_send(j, s, pr_ssem.at[i, s], sp, partner))

        slabs(one)

    def kv_arrive(i):
        level, part, up, down = route(i)
        mine = 4 * level + 2 * part + c
        with jax.named_scope("wait_kv"):
            slabs(lambda s: got(kv.at[mine, s], kv_rsem.at[mine, s]))
        kv_moves(i, lambda d: d.start())

    kv_arrive(0)
    kv_arrive(1)
    with jax.named_scope("ev_pre"):
        r0.forward()
        r0.near()
        r2.own()
        r3.own()
        r6.own(True)
    with jax.named_scope("wait_q"):
        for h in range(2):
            got(qb.at[h, 0], q_rsem.at[h, 0])
            got(lam.at[h], q_rsem.at[h, 2])

            @pl.when(large)
            def _():
                got(qb.at[h, 1], q_rsem.at[h, 1])
                qz[h, 0] = qb[h, 0]
                qz[h, 1] = qb[h, 1]

            @pl.when(jnp.logical_not(large))
            def _():
                both = qb[h, 0]
                first = lax.broadcasted_iota(jnp.int32, (CH, 128), 1) < 64
                qz[h, 0] = jnp.where(first, both, jnp.zeros_like(both))
                qz[h, 1] = jnp.where(first, jnp.zeros_like(both), both)

    def phase(i, carry):
        level, part, up, down = route(i)
        first = 4 * level + 2 * part
        other = first + 1 - c

        @pl.when(i >= 2)
        def _():
            kv_arrive(i)

        with jax.named_scope("ev_w"):
            @pl.when(i == 2)
            def _():
                r1.forward()

            @pl.when(i == 4)
            def _():
                r5.forward()
                r5.near()
                r7.own()
                r8.own()
                r0.far()
                r4.own()
                w_forward(w_f1)

            @pl.when(i == 6)
            def _():
                r2.forward()
                r3.forward()
                w_forward(w_f2)

        with jax.named_scope("wait_kv2"):
            slabs(lambda s: got(kv.at[other, s], kv_rsem.at[other, s]))
        n_lo = jnp.clip(lo_chunk - first + 1, 0, 2)
        n_hi = jnp.clip(hi_chunk - first + 1, 0, 2)

        def step(k, cc):
            h = jnp.where(k >= n_lo, 1, 0)
            j = first + k - h * n_lo
            diagonal = j == jnp.where(h == 1, hi_chunk, lo_chunk)

            @pl.when(diagonal)
            def _():
                absorb(h, j, True)

            @pl.when(jnp.logical_not(diagonal))
            def _():
                absorb(h, j, False)

            return cc

        with jax.named_scope("attn"):
            lax.fori_loop(0, n_lo + n_hi, step, 0)
        return carry

    lax.fori_loop(0, 8, phase, 0)

    slot = 8 * kind + 2 * y + x // 2
    for h in range(2):
        for t in range(2):
            rows = pl.ds(t * half, half)
            one = acc[h, 0, rows, 0:128] / acc[h, 0, rows, 128:256]
            two = acc[h, 1, rows, 0:128] / acc[h, 1, rows, 128:256]
            combined = one - lam[h, 0:1, :] * two
            square = jnp.mean(combined * combined, axis=1, keepdims=True)
            normed = combined * lax.rsqrt(square + norm_epsilon) * gain[...] * branch_scale
            ob[h, rows, :] = normed.astype(BF)
        dsp = hi_chunk if h == 1 else lo_chunk
        for t in range(8):
            put(ob.at[h, pl.ds(64 * t, 64), :], att.at[slot], o_ssem.at[h, t], o_rsem.at[slot], dsp, t)

    with jax.named_scope("ev_post"):
        r6.forward()
        r7.forward()
        r8.forward()
        r5.far()
        r9.own()
        r4.forward()
    with jax.named_scope("wait_wo"):
        w_forward(w_f3)
        pltpu.make_async_copy(osm, wo.at[own_a], l_sem.at[0]).wait()
        pltpu.make_async_copy(ola, wo.at[own_b], l_sem.at[1]).wait()
        for yy in (y, yu, yd, y2):
            for off in (0, 8):
                s = 2 * yy + 1 - c + off
                got(wo.at[s], w_rsem.at[s])
    with jax.named_scope("wait_att"):
        for s in range(16):
            got(att.at[s], o_rsem.at[s])
    rows = jnp.concatenate([att[s] for s in range(16)], axis=1)

    def project(n, carry):
        cols = pl.ds(pl.multiple_of(n * 512, 512), 512)
        w = wo[:, :, cols].reshape(2048, 512)
        pre[:, cols] = residual_scale * res[:, cols].astype(F32) + jnp.dot(
            rows, w, preferred_element_type=F32
        )
        return carry

    lax.fori_loop(0, 4, project, 0)
    values = pre[...]
    centered = values - jnp.mean(values, axis=1, keepdims=True)
    variance = jnp.mean(centered * centered, axis=1, keepdims=True)
    normed = (centered * lax.rsqrt(variance + norm_epsilon) * ngain[...]).astype(BF)
    nb[tp, 0] = normed[:, 0:1024]
    nb[tp, 1] = normed[:, 1024:2048]

    def n_send(t, k, ssem, dtp):
        return remote(nb.at[t, k], nb.at[t, k], ssem, n_rsem.at[t, k], sp, dtp)

    n_own = [
        n_send(tp, 0, nu_ssem.at[0], wu), n_send(tp, 1, nd_ssem.at[0], wd),
        n_send(tp, 1, nu_ssem.at[1], wu), n_send(tp, 0, nd_ssem.at[1], wd),
        n_send(tp, 0, np_ssem.at[0], partner), n_send(tp, 1, np_ssem.at[1], partner),
    ]
    n_fwd = [
        (wd, 0, [n_send(wd, 0, nu_ssem.at[2], wu), n_send(wd, 0, np_ssem.at[2], partner)]),
        (wu, 1, [n_send(wu, 1, nd_ssem.at[2], wd), n_send(wu, 1, np_ssem.at[3], partner)]),
        (wd, 1, [n_send(wd, 1, np_ssem.at[4], partner)]),
        (wu, 0, [n_send(wu, 0, np_ssem.at[5], partner)]),
        (w2, 0, [n_send(w2, 0, np_ssem.at[6], partner)]),
        (w2, 1, [n_send(w2, 1, np_ssem.at[7], partner)]),
    ]
    for d in n_own:
        d.start()
    with jax.named_scope("ev_post2"):
        r9.forward()
    with jax.named_scope("wait_nb"):
        for t, k, sends in n_fwd:
            got(nb.at[t, k], n_rsem.at[t, k])
            for d in sends:
                d.start()
    for n, a in enumerate((gw, uw, dw)):
        pltpu.make_async_copy(a, wt.at[sp, n], i_sem.at[6 + n]).wait()
    with jax.named_scope("wait_w"):
        for ring in (r1, r2, r3, r4, r6, r7, r8, r9):
            ring.near()
            ring.far()

    def mixer(groups):
        rows = []
        for g, yy in groups:
            t = 2 * yy + 1 - c
            got(nb.at[t, 0], n_rsem.at[t, 0])
            got(nb.at[t, 1], n_rsem.at[t, 1])
            for t in (2 * yy + 1 - c, 2 * yy + c):
                rows.append(jnp.concatenate([nb[t, 0], nb[t, 1]], axis=1))
        rows = jnp.concatenate(rows, axis=0)
        nt = (((1,), (1,)), ((), ()))
        gate = lax.dot_general(
            rows, jnp.concatenate([wt[s, 0] for s in range(16)], axis=1), nt, preferred_element_type=F32
        )
        up = lax.dot_general(
            rows, jnp.concatenate([wt[s, 1] for s in range(16)], axis=1), nt, preferred_element_type=F32
        )
        hidden = (gate / (1.0 + jnp.exp(-gate)) * up).astype(BF)
        for n in range(8):
            cols = pl.ds(256 * n, 256)
            w = jnp.concatenate([wt[2 * n, 2], wt[2 * n + 1, 2]], axis=1)
            part = jnp.dot(hidden, w, preferred_element_type=F32)
            for at, (g, yy) in enumerate(groups):
                psend[g, :, cols] = part[128 * at : 128 * at + 64].astype(BF)
                mine_f[g, :, cols] = part[128 * at + 64 : 128 * at + 128]
        for g, yy in groups:
            p_move(g).start()

    def p_move(g):
        return remote(psend.at[g], precv.at[g], p_ssem.at[g], p_rsem.at[g], sp, partner)

    def pair_sum(g):
        got(precv.at[g], p_rsem.at[g])
        both = (mine_f[g] + precv[g].astype(F32)).astype(BF)
        rsend[g, 0] = both[:, 0:1024]
        rsend[g, 1] = both[:, 1024:2048]

    r_up = remote(rsend.at[1], rrecv.at[0], r_ssem.at[0], r_rsem.at[0], sp, wu)
    r_down = remote(rsend.at[2], rrecv.at[1], r_ssem.at[1], r_rsem.at[1], sp, wd)
    r_a = remote(rsend.at[0, 0], tbuf.at[0], r_ssem.at[2], t_rsem.at[0], sp, wu)
    r_b = remote(rsend.at[0, 1], tbuf.at[1], r_ssem.at[3], t_rsem.at[1], sp, wd)
    f_a = remote(tbuf.at[0], rrecv.at[2, 0], r_ssem.at[4], r_rsem.at[2], sp, wu)
    f_b = remote(tbuf.at[1], rrecv.at[2, 1], r_ssem.at[5], r_rsem.at[3], sp, wd)
    with jax.named_scope("mix0"):
        mixer([(0, y2)])
    with jax.named_scope("pair0"):
        pair_sum(0)
        r_a.start()
        r_b.start()
    with jax.named_scope("mix1"):
        mixer([(1, yu), (2, yd)])
    with jax.named_scope("pair12"):
        got(tbuf.at[0], t_rsem.at[0])
        f_a.start()
        got(tbuf.at[1], t_rsem.at[1])
        f_b.start()
        pair_sum(1)
        r_up.start()
        pair_sum(2)
        r_down.start()
    mixer_own = [(3, y)]
    with jax.named_scope("mix3"):
        mixer(mixer_own)
    got(precv.at[3], p_rsem.at[3])
    pre[...] = residual_scale * normed.astype(F32) + 0.5 * (mine_f[3] + precv[3].astype(F32))
    with jax.named_scope("wait_r"):
        got(rrecv.at[0], r_rsem.at[0])
        got(rrecv.at[1], r_rsem.at[1])
        got(rrecv.at[2, 0], r_rsem.at[2])
        got(rrecv.at[2, 1], r_rsem.at[3])
    for k in range(2):
        cols = pl.ds(1024 * k, 1024)
        more = rrecv[0, k].astype(F32) + rrecv[1, k].astype(F32) + rrecv[2, k].astype(F32)
        out[:, cols] = (pre[:, cols] + 0.5 * more).astype(BF)

    for p in kv_puts:
        put_done(*p)
    for p in q_puts:
        put_done(*p)
    for d in w_own:
        d.wait_send()
    for item in w_f1 + w_f2 + w_f3:
        for d in item[1:]:
            d.wait_send()

    for ring in (r0, r1, r2, r3, r4, r5, r6, r7, r8, r9):
        ring.drain()
    for d in n_own:
        d.wait_send()
    for t, k, sends in n_fwd:
        for d in sends:
            d.wait_send()
    for g in range(4):
        p_move(g).wait_send()
    for d in (r_up, r_down, r_a, r_b, f_a, f_b):
        d.wait_send()

    def drain(i, carry):
        kv_moves(i, lambda d: d.wait_send())
        return carry

    lax.fori_loop(0, 8, drain, 0)
    for h in range(2):
        dsp = hi_chunk if h == 1 else lo_chunk
        for t in range(8):
            put_done(ob.at[h, pl.ds(64 * t, 64), :], att.at[slot], o_ssem.at[h, t], o_rsem.at[slot], dsp, t)


def block(*args):
    dma = pltpu.SemaphoreType.DMA
    return pl.pallas_call(
        block_kernel,
        name="block",
        out_shape=jax.ShapeDtypeStruct((64, 2048), BF),
        in_specs=[
            pl.BlockSpec(memory_space=pl.ANY if n in (0, 1, 2, 3, 4, 5, 8, 9, 12, 13, 14) else pltpu.VMEM)
            for n in range(len(args))
        ],
        out_specs=pl.BlockSpec(memory_space=pltpu.VMEM),
        scratch_shapes=[
            pltpu.VMEM((CH, 128), BF), pltpu.VMEM((CH, 256), BF), pltpu.VMEM((CH, 128), BF),
            pltpu.VMEM((CH, 256), BF), pltpu.VMEM((CH, 128), BF), pltpu.VMEM((CH, 128), BF),
            pltpu.VMEM((16, 3, CH, 128), BF),
            pltpu.VMEM((2, 2, CH, 128), BF),
            pltpu.VMEM((2, 2, CH, 128), BF),
            pltpu.VMEM((2, 8, 128), F32),
            pltpu.VMEM((2, 2, CH, 256), F32),
            pltpu.VMEM((2, 2, CH, 128), F32),
            pltpu.VMEM((16, 128, 2048), BF),
            pltpu.VMEM((2, CH, 128), BF),
            pltpu.VMEM((16, 64, 128), BF),
            pltpu.VMEM((64, 2048), F32),
            pltpu.VMEM((16, 3, 704, 128), BF),
            pltpu.VMEM((8, 2, 64, 1024), BF),
            pltpu.VMEM((4, 64, 2048), BF),
            pltpu.VMEM((4, 64, 2048), BF),
            pltpu.VMEM((4, 64, 2048), F32),
            pltpu.VMEM((3, 2, 64, 1024), BF),
            pltpu.VMEM((3, 2, 64, 1024), BF),
            pltpu.VMEM((2, 64, 1024), BF),
            dma((5,)), dma((2, 3)), dma((5,)), dma((16, 3)), dma((3, 3)), dma((3, 3)), dma((8, 3)),
            dma((3,)), dma((3,)), dma((8,)), dma((16,)), dma((2, 8)), dma((16,)), dma((2,)),
            dma((10, 6)), dma((16, 4)), dma((3,)), dma((3,)), dma((8,)), dma((8, 2)),
            dma((4,)), dma((4,)), dma((6,)), dma((4,)), dma((2,)), dma((9,)),
        ],
        compiler_params=pltpu.CompilerParams(has_side_effects=True, collective_id=0, vmem_limit_bytes=60 * 1024 * 1024),
        cost_estimate=pl.CostEstimate(flops=8 * 10**9, bytes_accessed=10**8, transcendentals=10**7),
    )(*args)


def per_device(
    residual, query_small, key_small, value_small, query_large, key_large, value_large,
    lambda_small, lambda_large, head_gain, output_small, output_large, norm_gain,
    gate_weight, up_weight, down_weight,
):
    flat = lambda a: a.reshape(a.shape[0], a.shape[2])
    lam = jnp.broadcast_to(jnp.stack([lambda_small, lambda_large]).reshape(2, 1, 1), (2, 8, 128))
    return block(
        flat(query_small), flat(query_large), flat(key_small), flat(key_large), flat(value_small),
        flat(value_large), lam, head_gain.reshape(1, 128), output_small, output_large, residual,
        norm_gain.reshape(1, 2048), gate_weight.T, up_weight.T, down_weight,
    )


def solution(mesh):
    in_specs = (
        P(("sp", "tp"), None),
        P("sp", "tp", None), P("sp", "tp", None), P("sp", "tp", None),
        P("sp", "tp", None), P("sp", "tp", None), P("sp", "tp", None),
        P("tp"), P("tp"), P(), P("tp", None), P("tp", None), P(),
        P("sp", "tp"), P("sp", "tp"), P("tp", "sp"),
    )
    return jax.shard_map(
        per_device, mesh=mesh, in_specs=in_specs, out_specs=P(("sp", "tp"), None), check_vma=False
    )
```

```python
import math

import jax
import jax.numpy as jnp
from jax import lax
from jax.experimental import pallas as pl
from jax.experimental.pallas import tpu as pltpu
from jax.sharding import PartitionSpec as P

residual_scale = 8.0**0.25
branch_scale = 0.8
norm_epsilon = 1e-05
masked_score = -1e30
log2e = math.log2(math.e)
MESH = pl.DeviceIdType.MESH
BF = jnp.bfloat16
F32 = jnp.float32
CH = 512


def remote(src, dst, ssem, rsem, sp, tp):
    return pltpu.make_async_remote_copy(
        src_ref=src, dst_ref=dst, send_sem=ssem, recv_sem=rsem, device_id=(sp, tp), device_id_type=MESH
    )


def block_kernel(
    qs_in, ql_in, ks_in, kl_in, vs_in, vl_in, lam_s, lam_l, gain, osm, ola, res, ngain, gw, uw, dw,
    out,
    qs, ql, ks, kl, vs, vl, lam_in, kv, qb, qz, lam, acc, mx, wo, ob, att, pre, wt, nb, psend, precv, mine_f, rsend, rrecv, tbuf, rbuf,
    q_ssem, q_rsem, x_ssem, kv_rsem, up_ssem, dn_ssem, pr_ssem,
    wu_ssem, wd_ssem, wp_ssem, w_rsem, o_ssem, o_rsem, l_sem,
    g_ssem, g_rsem, nu_ssem, nd_ssem, np_ssem, n_rsem, p_ssem, p_rsem, r_ssem, r_rsem, t_rsem, i_sem, relay_sem,
):
    sp, tp = lax.axis_index("sp"), lax.axis_index("tp")
    z, x, y, c = sp // 4, sp % 4, tp // 2, tp % 2
    kind = x % 2
    large = kind == 1
    zu, zd, z2 = (z + 1) % 4, (z + 3) % 4, (z + 2) % 4
    yu, yd, y2 = (y + 1) % 4, (y + 3) % 4, (y + 2) % 4
    xu, xd, x2 = (x + 1) % 4, (x + 3) % 4, (x + 2) % 4
    r = 2 * (3 - z) + c
    lo_chunk, hi_chunk = r, 15 - r

    def put(src, dst, ssem, rsem, dsp, dtp):
        same = jnp.logical_and(dsp == sp, dtp == tp)

        @pl.when(same)
        def _():
            pltpu.make_async_copy(src, dst, rsem).start()

        @pl.when(jnp.logical_not(same))
        def _():
            remote(src, dst, ssem, rsem, dsp, dtp).start()

    def put_done(src, dst, ssem, rsem, dsp, dtp):
        same = jnp.logical_and(dsp == sp, dtp == tp)

        @pl.when(jnp.logical_not(same))
        def _():
            remote(src, dst, ssem, rsem, dsp, dtp).wait_send()

    def got(dst, rsem):
        pltpu.make_async_copy(dst, dst, rsem).wait()

    staged = [
        pltpu.make_async_copy(a, b, i_sem.at[n])
        for n, (a, b) in enumerate(
            ((ks_in, ks), (vs_in, vs), (kl_in, kl), (vl_in, vl), (qs_in, qs), (ql_in, ql))
        )
    ]
    for d in staged:
        d.start()
    lam_in[0] = jnp.full((8, 128), lam_s[0], F32)
    lam_in[1] = jnp.full((8, 128), lam_l[0], F32)
    dcore = 2 * y + x % 2
    small_sp, large_sp = 4 * z + 2 * c, 4 * z + 2 * c + 1
    kv_puts = [
        (ks, kv.at[sp, 0], x_ssem.at[0], kv_rsem.at[sp, 0], small_sp, dcore),
        (vs, kv.at[sp, 1], x_ssem.at[1], kv_rsem.at[sp, 1], small_sp, dcore),
        (kl.at[:, pl.ds(0, 128)], kv.at[sp, 0], x_ssem.at[2], kv_rsem.at[sp, 0], large_sp, dcore),
        (vl, kv.at[sp, 1], x_ssem.at[3], kv_rsem.at[sp, 1], large_sp, dcore),
        (kl.at[:, pl.ds(128, 128)], kv.at[sp, 2], x_ssem.at[4], kv_rsem.at[sp, 2], large_sp, dcore),
    ]
    two_away = (2 * c + 5 - x) % 4 == 2
    relays = x == 2 * c
    through = [
        remote(p[0], rbuf.at[k], p[2], relay_sem.at[k], 4 * z + xu, tp) for k, p in enumerate(kv_puts[2:])
    ]
    onward = [
        remote(rbuf.at[k], kv.at[4 * z + xd, b], relay_sem.at[3 + k], kv_rsem.at[4 * z + xd, b], 4 * z + xu, 2 * y + 1)
        for k, b in enumerate((0, 1, 2))
    ]
    low = jnp.minimum(sp, 15 - sp)
    hi = sp // 8
    qsp = 4 * (3 - low // 2) + 2 * c
    qtp = 2 * y + low % 2
    q_puts = [
        (qs, qb.at[hi, 0], q_ssem.at[0], q_rsem.at[hi, 0], qsp, qtp),
        (ql.at[:, pl.ds(0, 128)], qb.at[hi, 0], q_ssem.at[1], q_rsem.at[hi, 0], qsp + 1, qtp),
        (ql.at[:, pl.ds(128, 128)], qb.at[hi, 1], q_ssem.at[2], q_rsem.at[hi, 1], qsp + 1, qtp),
        (lam_in.at[0], lam.at[hi], q_ssem.at[3], q_rsem.at[hi, 2], qsp, qtp),
        (lam_in.at[1], lam.at[hi], q_ssem.at[4], q_rsem.at[hi, 2], qsp + 1, qtp),
    ]
    barrier = pltpu.get_barrier_semaphore()

    def greet(dsp, dtp):
        @pl.when(jnp.logical_not(jnp.logical_and(dsp == sp, dtp == tp)))
        def _():
            pl.semaphore_signal(barrier, inc=1, device_id=(dsp, dtp), device_id_type=MESH)

    sources = [(4 * z + c, 2 * y + x // 2), (4 * z + c + 2, 2 * y + x // 2)]
    targets = [(small_sp, dcore), (large_sp, dcore)]
    sources += [(lo_chunk, 2 * y + x // 2), (hi_chunk, 2 * y + x // 2)]
    targets += [(qsp, qtp), (qsp + 1, qtp)]
    near = [(4 * zu + x, tp), (4 * zd + x, tp), (4 * z + xu, tp), (4 * z + xd, tp)]
    near += [(sp, 2 * yu + c), (sp, 2 * yd + c), (sp, 2 * y + 1 - c)]
    sources += near + [(4 * (3 - low // 2) + a, 2 * b + low % 2) for a in range(4) for b in range(4)]
    targets += near + [(a, t) for a in (lo_chunk, hi_chunk) for t in range(8)]
    for d in sources:
        greet(*d)

    @pl.when(jnp.logical_and(large, c == 1))
    def _():
        greet(4 * z + xd, 2 * y + x // 2)

    count = len(targets) + relays.astype(jnp.int32)
    for d in targets:
        count -= jnp.logical_and(d[0] == sp, d[1] == tp).astype(jnp.int32)
    with jax.named_scope("barrier"):
        pl.semaphore_wait(barrier, count)
    for d in staged:
        d.wait()

    @pl.when(two_away)
    def _():
        for d in through:
            d.start()

    @pl.when(jnp.logical_not(two_away))
    def _():
        for p in kv_puts[2:]:
            put(*p)

    for p in q_puts[1:3] + q_puts[4:] + kv_puts[:2] + q_puts[:1] + q_puts[3:4]:
        put(*p)

    own_piece = (gw, uw, dw.at[pl.ds(0, 352), :], dw.at[pl.ds(352, 352), :])

    def piece(s, k):
        return wt.at[s, k] if k < 2 else wt.at[s, 2, pl.ds(352 * (k - 2), 352), :]

    class Ring:
        def __init__(self, at, along_x, first, line):
            self.at, self.first = at, first
            if along_x:
                self.slots = [4 * line + p for p in (x, xd, xu, x2)]
                self.up, self.down = 4 * z + xu, 4 * z + xd
            else:
                self.slots = [4 * p + line for p in (z, zd, zu, z2)]
                self.up, self.down = 4 * zu + x, 4 * zd + x

        def send(self, n, which, k, to, src=None):
            s = self.slots[which]
            ref = piece(s, k)
            return remote(ref if src is None else src, ref, g_ssem.at[self.at, n], g_rsem.at[s, k], to, tp)

        def own_sends(self, from_input=False):
            a, b = self.first, self.first + 1
            sa, sb = (own_piece[a], own_piece[b]) if from_input else (None, None)
            return [
                self.send(0, 0, a, self.up, sa), self.send(1, 0, b, self.down, sb),
                self.send(2, 0, b, self.up, sb), self.send(3, 0, a, self.down, sa),
            ]

        def far_sends(self):
            return self.send(4, 1, self.first, self.up), self.send(5, 2, self.first + 1, self.down)

        def got(self, which, k):
            got(piece(self.slots[which], k), g_rsem.at[self.slots[which], k])

        def own(self, from_input=False):
            for d in self.own_sends(from_input):
                d.start()

        def forward(self):
            f1, f2 = self.far_sends()
            self.got(1, self.first)
            f1.start()
            self.got(2, self.first + 1)
            f2.start()

        def near(self):
            self.got(1, self.first + 1)
            self.got(2, self.first)

        def far(self):
            self.got(3, self.first)
            self.got(3, self.first + 1)

        def drain(self):
            for d in (*self.own_sends(), *self.far_sends()):
                d.wait_send()

    r0 = Ring(0, False, 0, x)
    r1, r2, r3, r4 = [Ring(1 + n, True, 0, line) for n, line in enumerate((z, zd, zu, z2))]
    r5 = Ring(5, True, 2, z)
    r6, r7, r8, r9 = [Ring(6 + n, False, 2, line) for n, line in enumerate((x, xd, xu, x2))]
    r0.own(True)

    @pl.when(relays)
    def _():
        for k, d in enumerate(onward):
            got(rbuf.at[k], relay_sem.at[k])
            d.start()

    for ring in (r5, r1):
        ring.own(True)

    wu, wd = 2 * yu + c, 2 * yd + c
    partner = 2 * y + 1 - c

    def w_send(slot, ssem, dtp, src=None):
        ref = wo.at[slot]
        return remote(ref if src is None else src, ref, ssem, w_rsem.at[slot], sp, dtp)

    own_a, own_b = tp, 8 + tp
    w_own = [
        w_send(own_a, wu_ssem.at[0], wu, osm), w_send(own_b, wd_ssem.at[0], wd, ola),
        w_send(own_b, wu_ssem.at[1], wu, ola), w_send(own_a, wd_ssem.at[1], wd, osm),
        w_send(own_a, wp_ssem.at[0], partner, osm), w_send(own_b, wp_ssem.at[1], partner, ola),
    ]
    for d in w_own:
        d.start()
    pltpu.make_async_copy(osm, wo.at[own_a], l_sem.at[0]).start()
    pltpu.make_async_copy(ola, wo.at[own_b], l_sem.at[1]).start()
    fwd_a, fwd_b = wd, 8 + wu
    w_f1 = [
        (fwd_a, w_send(fwd_a, wu_ssem.at[2], wu), w_send(fwd_a, wp_ssem.at[2], partner)),
        (fwd_b, w_send(fwd_b, wd_ssem.at[2], wd), w_send(fwd_b, wp_ssem.at[3], partner)),
    ]
    w_f2 = [
        (8 + wd, w_send(8 + wd, wp_ssem.at[4], partner)),
        (wu, w_send(wu, wp_ssem.at[5], partner)),
    ]
    w2 = 2 * y2 + c
    w_f3 = [
        (w2, w_send(w2, wp_ssem.at[6], partner)),
        (8 + w2, w_send(8 + w2, wp_ssem.at[7], partner)),
    ]

    def w_forward(items):
        for item in items:
            got(wo.at[item[0]], w_rsem.at[item[0]])
            for d in item[1:]:
                d.start()

    for n, a in enumerate((gw, uw, dw)):
        pltpu.make_async_copy(a, wt.at[sp, n], i_sem.at[6 + n]).start()
    acc[...] = jnp.zeros_like(acc)
    mx[...] = jnp.full_like(mx, masked_score)

    factor = jnp.where(large, log2e * 128**-0.5, log2e * 64**-0.5).astype(F32)
    half = CH // 2

    def absorb(h, first, shift):
        subs = [(m, t) for m in range(2) for t in range(2)]
        values = jnp.concatenate(
            [jnp.concatenate([kv[first + a, 1], jnp.ones((CH, 128), BF)], axis=1) for a in range(2)], axis=0
        )

        def scores(m, t):
            found = []
            for a in range(2):
                s = lax.dot_general(
                    qz[h, m, pl.ds(t * half, half), :], kv[first + a, 2 * m * kind],
                    (((1,), (1,)), ((), ())), preferred_element_type=F32,
                )
                if shift is not None:
                    qi = lax.broadcasted_iota(jnp.int32, (half, CH), 0) + (shift + t * half)
                    ki = lax.broadcasted_iota(jnp.int32, (half, CH), 1) + a * CH
                    s = jnp.where(ki <= qi, s, masked_score)
                found.append(s)
            return found, jnp.max(jnp.maximum(found[0], found[1]), axis=1, keepdims=True)

        now = scores(*subs[0])
        for i, (m, t) in enumerate(subs):
            later = scores(*subs[i + 1]) if i < 3 else None
            rows = pl.ds(t * half, half)
            old = mx[h, m, rows, :]
            new = jnp.maximum(old, now[1])
            mx[h, m, rows, :] = new
            wide = jnp.concatenate([new] * 4, axis=1)
            p = jnp.concatenate([jnp.exp2((s - wide) * factor).astype(BF) for s in now[0]], axis=1)
            fade = jnp.exp2((old - new) * factor)
            pv = jnp.dot(p, values, preferred_element_type=F32)
            acc[h, m, rows, 0:128] = acc[h, m, rows, 0:128] * fade + pv[:, 0:128]
            acc[h, m, rows, 128:256] = acc[h, m, rows, 128:256] * fade + pv[:, 128:256]
            now = later

    def kv_send(j, slab, ssem, dsp, dtp):
        return remote(kv.at[j, slab], kv.at[j, slab], ssem, kv_rsem.at[j, slab], dsp, dtp)

    def slabs(fn):
        fn(0)
        fn(1)

        @pl.when(large)
        def _():
            fn(2)

    def route(i):
        own = i < 2
        off = jnp.where(own, 0, jnp.where((i == 2) | (i == 4), 3, jnp.where(i < 6, 1, 2)))
        part = jnp.where((i == 0) | (i == 2) | (i == 5) | (i == 6), 0, 1)
        level = (z + off) % 4
        up = own | (i == 2)
        down = own | (i == 3)
        return level, part, up, down

    def kv_moves(i, act):
        level, part, up, down = route(i)
        j = 4 * level + 2 * part + c

        def one(s):
            @pl.when(up)
            def _():
                act(kv_send(j, s, up_ssem.at[jnp.minimum(i, 2), s], 4 * zu + x, tp))

            @pl.when(down)
            def _():
                act(kv_send(j, s, dn_ssem.at[jnp.minimum(i, 2), s], 4 * zd + x, tp))

            act(kv_send(j, s, pr_ssem.at[i, s], sp, partner))

        slabs(one)

    def kv_arrive(i):
        level, part, up, down = route(i)
        mine = 4 * level + 2 * part + c
        with jax.named_scope("wait_kv"):
            slabs(lambda s: got(kv.at[mine, s], kv_rsem.at[mine, s]))
        kv_moves(i, lambda d: d.start())

    kv_arrive(0)
    kv_arrive(1)
    with jax.named_scope("wait_q"):
        for h in range(2):
            got(qb.at[h, 0], q_rsem.at[h, 0])
            got(lam.at[h], q_rsem.at[h, 2])

            @pl.when(large)
            def _():
                got(qb.at[h, 1], q_rsem.at[h, 1])
                qz[h, 0] = qb[h, 0]
                qz[h, 1] = qb[h, 1]

            @pl.when(jnp.logical_not(large))
            def _():
                both = qb[h, 0]
                first = lax.broadcasted_iota(jnp.int32, (CH, 128), 1) < 64
                qz[h, 0] = jnp.where(first, both, jnp.zeros_like(both))
                qz[h, 1] = jnp.where(first, jnp.zeros_like(both), both)


    def phase(i, carry):
        level, part, up, down = route(i)
        first = 4 * level + 2 * part
        other = first + 1 - c

        @pl.when((i >= 1) & (i < 7))
        def _():
            kv_arrive(i + 1)

        with jax.named_scope("ev_w"):
            @pl.when(i == 1)
            def _():
                r0.forward()
                r5.forward()
                r0.near()
                r2.own()
                r3.own()

            @pl.when(i == 2)
            def _():
                w_forward(w_f1)

            @pl.when(i == 4)
            def _():
                r6.own(True)
                w_forward(w_f2)

            @pl.when(i == 6)
            def _():
                w_forward(w_f3)

        with jax.named_scope("wait_kv2"):
            slabs(lambda s: got(kv.at[other, s], kv_rsem.at[other, s]))
        n_lo = jnp.where(lo_chunk >= first, 1, 0)
        n_hi = jnp.where(hi_chunk >= first, 1, 0)

        def step(k, cc):
            h = jnp.where(k >= n_lo, 1, 0)
            gap = jnp.where(h == 1, hi_chunk, lo_chunk) - first

            @pl.when(gap < 2)
            def _():
                absorb(h, first, gap * CH)

            @pl.when(gap >= 2)
            def _():
                absorb(h, first, None)

            return cc

        with jax.named_scope("attn"):
            lax.fori_loop(0, n_lo + n_hi, step, 0)
        return carry

    lax.fori_loop(0, 8, phase, 0)

    slot = 8 * kind + 2 * y + x // 2
    for h in range(2):
        for t in range(2):
            rows = pl.ds(t * half, half)
            one = acc[h, 0, rows, 0:128] / acc[h, 0, rows, 128:256]
            two = acc[h, 1, rows, 0:128] / acc[h, 1, rows, 128:256]
            combined = one - lam[h, 0:1, :] * two
            square = jnp.mean(combined * combined, axis=1, keepdims=True)
            normed = combined * lax.rsqrt(square + norm_epsilon) * gain[...] * branch_scale
            ob[h, rows, :] = normed.astype(BF)
        dsp = hi_chunk if h == 1 else lo_chunk
        for t in range(8):
            put(ob.at[h, pl.ds(64 * t, 64), :], att.at[slot], o_ssem.at[h, t], o_rsem.at[slot], dsp, t)

    with jax.named_scope("ev_post"):
        r0.far()
        r4.own()
        r5.near()
        r7.own()
        r8.own()
        r5.far()
        r9.own()
        r1.forward()
        r2.forward()
        r3.forward()
        r6.forward()
    with jax.named_scope("wait_wo"):
        pltpu.make_async_copy(osm, wo.at[own_a], l_sem.at[0]).wait()
        pltpu.make_async_copy(ola, wo.at[own_b], l_sem.at[1]).wait()
        for yy in (y, yu, yd, y2):
            for off in (0, 8):
                s = 2 * yy + 1 - c + off
                got(wo.at[s], w_rsem.at[s])
    with jax.named_scope("wait_att"):
        for s in range(16):
            got(att.at[s], o_rsem.at[s])
    rows = jnp.concatenate([att[s] for s in range(16)], axis=1)

    def project(n, carry):
        cols = pl.ds(pl.multiple_of(n * 512, 512), 512)
        w = wo[:, :, cols].reshape(2048, 512)
        pre[:, cols] = residual_scale * res[:, cols].astype(F32) + jnp.dot(
            rows, w, preferred_element_type=F32
        )
        return carry

    lax.fori_loop(0, 4, project, 0)
    values = pre[...]
    centered = values - jnp.mean(values, axis=1, keepdims=True)
    variance = jnp.mean(centered * centered, axis=1, keepdims=True)
    normed = (centered * lax.rsqrt(variance + norm_epsilon) * ngain[...]).astype(BF)
    nb[tp, 0] = normed[:, 0:1024]
    nb[tp, 1] = normed[:, 1024:2048]

    def n_send(t, k, ssem, dtp):
        return remote(nb.at[t, k], nb.at[t, k], ssem, n_rsem.at[t, k], sp, dtp)

    n_own = [
        n_send(tp, 0, nu_ssem.at[0], wu), n_send(tp, 1, nd_ssem.at[0], wd),
        n_send(tp, 1, nu_ssem.at[1], wu), n_send(tp, 0, nd_ssem.at[1], wd),
        n_send(tp, 0, np_ssem.at[0], partner), n_send(tp, 1, np_ssem.at[1], partner),
    ]
    n_fwd = [
        (wd, 0, [n_send(wd, 0, nu_ssem.at[2], wu), n_send(wd, 0, np_ssem.at[2], partner)]),
        (wu, 1, [n_send(wu, 1, nd_ssem.at[2], wd), n_send(wu, 1, np_ssem.at[3], partner)]),
        (wd, 1, [n_send(wd, 1, np_ssem.at[4], partner)]),
        (wu, 0, [n_send(wu, 0, np_ssem.at[5], partner)]),
        (w2, 0, [n_send(w2, 0, np_ssem.at[6], partner)]),
        (w2, 1, [n_send(w2, 1, np_ssem.at[7], partner)]),
    ]
    for d in n_own:
        d.start()
    def n_forward(items):
        for t, k, sends in items:
            got(nb.at[t, k], n_rsem.at[t, k])
            for d in sends:
                d.start()

    with jax.named_scope("ev_post2"):
        r7.forward()
        r8.forward()
        r4.forward()
    with jax.named_scope("wait_nb0"):
        n_forward(n_fwd[:2])
    with jax.named_scope("ev_post3"):
        r9.forward()
    with jax.named_scope("wait_nb"):
        n_forward(n_fwd[2:])
    for n, a in enumerate((gw, uw, dw)):
        pltpu.make_async_copy(a, wt.at[sp, n], i_sem.at[6 + n]).wait()
    with jax.named_scope("wait_w"):
        for ring in (r1, r2, r3, r4, r6, r7, r8, r9):
            ring.near()
            ring.far()

    def mixer(groups):
        rows = []
        for g, yy in groups:
            t = 2 * yy + 1 - c
            got(nb.at[t, 0], n_rsem.at[t, 0])
            got(nb.at[t, 1], n_rsem.at[t, 1])
            for t in (2 * yy + 1 - c, 2 * yy + c):
                rows.append(jnp.concatenate([nb[t, 0], nb[t, 1]], axis=1))
        rows = jnp.concatenate(rows, axis=0)
        nt = (((1,), (1,)), ((), ()))
        gate = lax.dot_general(
            rows, jnp.concatenate([wt[s, 0] for s in range(16)], axis=1), nt, preferred_element_type=F32
        )
        up = lax.dot_general(
            rows, jnp.concatenate([wt[s, 1] for s in range(16)], axis=1), nt, preferred_element_type=F32
        )
        hidden = (gate / (1.0 + jnp.exp(-gate)) * up).astype(BF)
        for n in range(8):
            cols = pl.ds(256 * n, 256)
            w = jnp.concatenate([wt[2 * n, 2], wt[2 * n + 1, 2]], axis=1)
            part = jnp.dot(hidden, w, preferred_element_type=F32)
            for at, (g, yy) in enumerate(groups):
                psend[g, :, cols] = part[128 * at : 128 * at + 64].astype(BF)
                mine_f[g, :, cols] = part[128 * at + 64 : 128 * at + 128]
        for g, yy in groups:
            p_move(g).start()

    def p_move(g):
        return remote(psend.at[g], precv.at[g], p_ssem.at[g], p_rsem.at[g], sp, partner)

    def pair_sum(g, k):
        cols = pl.ds(1024 * k, 1024)
        return mine_f[g, :, cols] + precv[g, :, cols].astype(F32)

    r_a = remote(rsend.at[0, 0], tbuf.at[0], r_ssem.at[0], t_rsem.at[0], sp, wu)
    r_b = remote(rsend.at[0, 1], tbuf.at[1], r_ssem.at[1], t_rsem.at[1], sp, wd)
    up_a = remote(rsend.at[1, 0], rrecv.at[0, 0], r_ssem.at[2], r_rsem.at[0], sp, wu)
    up_b = remote(rsend.at[1, 1], rrecv.at[0, 1], r_ssem.at[3], r_rsem.at[1], sp, wu)
    down_a = remote(rsend.at[2, 0], rrecv.at[1, 0], r_ssem.at[4], r_rsem.at[2], sp, wd)
    down_b = remote(rsend.at[2, 1], rrecv.at[1, 1], r_ssem.at[5], r_rsem.at[3], sp, wd)
    with jax.named_scope("mix0"):
        mixer([(0, y2)])
    with jax.named_scope("pair0"):
        got(precv.at[0], p_rsem.at[0])
        rsend[0, 0] = pair_sum(0, 0).astype(BF)
        r_a.start()
        rsend[0, 1] = pair_sum(0, 1).astype(BF)
        r_b.start()
    with jax.named_scope("mix1"):
        mixer([(1, yu), (2, yd)])
    with jax.named_scope("pair12"):
        got(precv.at[1], p_rsem.at[1])
        rsend[1, 1] = pair_sum(1, 1).astype(BF)
        up_b.start()
        got(precv.at[2], p_rsem.at[2])
        rsend[2, 0] = pair_sum(2, 0).astype(BF)
        down_a.start()
        got(tbuf.at[0], t_rsem.at[0])
        rsend[1, 0] = (pair_sum(1, 0) + tbuf[0].astype(F32)).astype(BF)
        up_a.start()
        got(tbuf.at[1], t_rsem.at[1])
        rsend[2, 1] = (pair_sum(2, 1) + tbuf[1].astype(F32)).astype(BF)
        down_b.start()
    with jax.named_scope("mix3"):
        mixer([(3, y)])
    got(precv.at[3], p_rsem.at[3])
    pre[...] = residual_scale * normed.astype(F32) + 0.5 * (mine_f[3] + precv[3].astype(F32))
    with jax.named_scope("wait_r"):
        for k in range(2):
            got(rrecv.at[0, k], r_rsem.at[k])
            got(rrecv.at[1, k], r_rsem.at[2 + k])
    for k in range(2):
        cols = pl.ds(1024 * k, 1024)
        more = rrecv[0, k].astype(F32) + rrecv[1, k].astype(F32)
        out[:, cols] = (pre[:, cols] + 0.5 * more).astype(BF)

    @pl.when(two_away)
    def _():
        for d in through:
            d.wait_send()

    @pl.when(jnp.logical_not(two_away))
    def _():
        for p in kv_puts[2:]:
            put_done(*p)

    @pl.when(relays)
    def _():
        for d in onward:
            d.wait_send()

    for p in kv_puts[:2]:
        put_done(*p)
    for p in q_puts:
        put_done(*p)
    for d in w_own:
        d.wait_send()
    for item in w_f1 + w_f2 + w_f3:
        for d in item[1:]:
            d.wait_send()

    for ring in (r0, r1, r2, r3, r4, r5, r6, r7, r8, r9):
        ring.drain()
    for d in n_own:
        d.wait_send()
    for t, k, sends in n_fwd:
        for d in sends:
            d.wait_send()
    for g in range(4):
        p_move(g).wait_send()
    for d in (r_a, r_b, up_a, up_b, down_a, down_b):
        d.wait_send()

    def drain(i, carry):
        kv_moves(i, lambda d: d.wait_send())
        return carry

    lax.fori_loop(0, 8, drain, 0)
    for h in range(2):
        dsp = hi_chunk if h == 1 else lo_chunk
        for t in range(8):
            put_done(ob.at[h, pl.ds(64 * t, 64), :], att.at[slot], o_ssem.at[h, t], o_rsem.at[slot], dsp, t)


def block(*args):
    dma = pltpu.SemaphoreType.DMA
    return pl.pallas_call(
        block_kernel,
        name="block",
        out_shape=jax.ShapeDtypeStruct((64, 2048), BF),
        in_specs=[
            pl.BlockSpec(memory_space={"h": pl.ANY, "v": pltpu.VMEM, "s": pltpu.SMEM}[k])
            for k in "hhhhhhssvhhvvhhh"
        ],
        out_specs=pl.BlockSpec(memory_space=pltpu.VMEM),
        scratch_shapes=[
            pltpu.VMEM((CH, 128), BF), pltpu.VMEM((CH, 256), BF), pltpu.VMEM((CH, 128), BF),
            pltpu.VMEM((CH, 256), BF), pltpu.VMEM((CH, 128), BF), pltpu.VMEM((CH, 128), BF),
            pltpu.VMEM((2, 8, 128), F32),
            pltpu.VMEM((16, 3, CH, 128), BF),
            pltpu.VMEM((2, 2, CH, 128), BF),
            pltpu.VMEM((2, 2, CH, 128), BF),
            pltpu.VMEM((2, 8, 128), F32),
            pltpu.VMEM((2, 2, CH, 256), F32),
            pltpu.VMEM((2, 2, CH, 128), F32),
            pltpu.VMEM((16, 128, 2048), BF),
            pltpu.VMEM((2, CH, 128), BF),
            pltpu.VMEM((16, 64, 128), BF),
            pltpu.VMEM((64, 2048), F32),
            pltpu.VMEM((16, 3, 704, 128), BF),
            pltpu.VMEM((8, 2, 64, 1024), BF),
            pltpu.VMEM((4, 64, 2048), BF),
            pltpu.VMEM((4, 64, 2048), BF),
            pltpu.VMEM((4, 64, 2048), F32),
            pltpu.VMEM((3, 2, 64, 1024), BF),
            pltpu.VMEM((2, 2, 64, 1024), BF),
            pltpu.VMEM((2, 64, 1024), BF),
            pltpu.VMEM((3, CH, 128), BF),
            dma((5,)), dma((2, 3)), dma((5,)), dma((16, 3)), dma((3, 3)), dma((3, 3)), dma((8, 3)),
            dma((3,)), dma((3,)), dma((8,)), dma((16,)), dma((2, 8)), dma((16,)), dma((2,)),
            dma((10, 6)), dma((16, 4)), dma((3,)), dma((3,)), dma((8,)), dma((8, 2)),
            dma((4,)), dma((4,)), dma((6,)), dma((4,)), dma((2,)), dma((9,)), dma((6,)),
        ],
        compiler_params=pltpu.CompilerParams(has_side_effects=True, collective_id=0, vmem_limit_bytes=60 * 1024 * 1024),
        cost_estimate=pl.CostEstimate(flops=8 * 10**9, bytes_accessed=10**8, transcendentals=10**7),
    )(*args)


def per_device(
    residual, query_small, key_small, value_small, query_large, key_large, value_large,
    lambda_small, lambda_large, head_gain, output_small, output_large, norm_gain,
    gate_weight, up_weight, down_weight,
):
    flat = lambda a: a.reshape(a.shape[0], a.shape[2])
    return block(
        flat(query_small), flat(query_large), flat(key_small), flat(key_large), flat(value_small),
        flat(value_large), lambda_small, lambda_large, head_gain.reshape(1, 128), output_small, output_large, residual,
        norm_gain.reshape(1, 2048), gate_weight.T, up_weight.T, down_weight,
    )


def solution(mesh):
    in_specs = (
        P(("sp", "tp"), None),
        P("sp", "tp", None), P("sp", "tp", None), P("sp", "tp", None),
        P("sp", "tp", None), P("sp", "tp", None), P("sp", "tp", None),
        P("tp"), P("tp"), P(), P("tp", None), P("tp", None), P(),
        P("sp", "tp"), P("sp", "tp"), P("tp", "sp"),
    )
    return jax.shard_map(
        per_device, mesh=mesh, in_specs=in_specs, out_specs=P(("sp", "tp"), None), check_vma=False
    )
```

```python
import math

import jax
import jax.numpy as jnp
from jax import lax
from jax.experimental import pallas as pl
from jax.experimental.pallas import tpu as pltpu
from jax.sharding import PartitionSpec as P

residual_scale = 8.0**0.25
branch_scale = 0.8
norm_epsilon = 1e-05
masked_score = -1e30
log2e = math.log2(math.e)
MESH = pl.DeviceIdType.MESH
BF = jnp.bfloat16
F32 = jnp.float32
CH = 512


def remote(src, dst, ssem, rsem, sp, tp):
    return pltpu.make_async_remote_copy(
        src_ref=src, dst_ref=dst, send_sem=ssem, recv_sem=rsem, device_id=(sp, tp), device_id_type=MESH
    )


def block_kernel(
    qs_in, ql_in, ks_in, kl_in, vs_in, vl_in, lam_s, lam_l, gain_in, osm, ola, res_in, ngain_in, gw, uw, dw,
    out,
    qs, ql, ks, kl, vs, vl, lam_in, gain, res, ngain, kv, qb, qz, lam, acc, mx, wo, ob, att, pre, wt, nb, psend, precv, mine_f, rsend, rrecv, tbuf, rbuf,
    q_ssem, q_rsem, x_ssem, kv_rsem, up_ssem, dn_ssem, pr_ssem,
    wu_ssem, wd_ssem, wp_ssem, w_rsem, o_ssem, o_rsem, l_sem,
    g_ssem, g_rsem, nu_ssem, nd_ssem, np_ssem, n_rsem, p_ssem, p_rsem, r_ssem, r_rsem, t_rsem, i_sem, relay_sem,
):
    sp, tp = lax.axis_index("sp"), lax.axis_index("tp")
    z, x, y, c = sp // 4, sp % 4, tp // 2, tp % 2
    kind = x % 2
    large = kind == 1
    zu, zd, z2 = (z + 1) % 4, (z + 3) % 4, (z + 2) % 4
    yu, yd, y2 = (y + 1) % 4, (y + 3) % 4, (y + 2) % 4
    xu, xd, x2 = (x + 1) % 4, (x + 3) % 4, (x + 2) % 4
    r = 2 * jnp.where(z < 2, 3 - z, z - 2) + c
    lo_chunk, hi_chunk = r, 15 - r

    def put(src, dst, ssem, rsem, dsp, dtp):
        same = jnp.logical_and(dsp == sp, dtp == tp)

        @pl.when(same)
        def _():
            pltpu.make_async_copy(src, dst, rsem).start()

        @pl.when(jnp.logical_not(same))
        def _():
            remote(src, dst, ssem, rsem, dsp, dtp).start()

    def put_done(src, dst, ssem, rsem, dsp, dtp):
        same = jnp.logical_and(dsp == sp, dtp == tp)

        @pl.when(jnp.logical_not(same))
        def _():
            remote(src, dst, ssem, rsem, dsp, dtp).wait_send()

    def got(dst, rsem):
        pltpu.make_async_copy(dst, dst, rsem).wait()

    staged = [
        pltpu.make_async_copy(a, b, i_sem.at[n])
        for n, (a, b) in enumerate(
            ((ks_in, ks), (vs_in, vs), (kl_in, kl), (vl_in, vl), (qs_in, qs), (ql_in, ql))
        )
    ]
    for d in staged:
        d.start()
    small_in = [
        pltpu.make_async_copy(a, b, i_sem.at[9 + n])
        for n, (a, b) in enumerate(((gain_in, gain), (res_in, res), (ngain_in, ngain)))
    ]
    for d in small_in:
        d.start()
    lam_in[0] = jnp.full((8, 128), lam_s[0], F32)
    lam_in[1] = jnp.full((8, 128), lam_l[0], F32)
    dcore = 2 * y + x % 2
    small_sp, large_sp = 4 * z + 2 * c, 4 * z + 2 * c + 1
    kv_puts = [
        (ks, kv.at[sp, 0], x_ssem.at[0], kv_rsem.at[sp, 0], small_sp, dcore),
        (vs, kv.at[sp, 1], x_ssem.at[1], kv_rsem.at[sp, 1], small_sp, dcore),
        (kl.at[:, pl.ds(0, 128)], kv.at[sp, 0], x_ssem.at[2], kv_rsem.at[sp, 0], large_sp, dcore),
        (vl, kv.at[sp, 1], x_ssem.at[3], kv_rsem.at[sp, 1], large_sp, dcore),
        (kl.at[:, pl.ds(128, 128)], kv.at[sp, 2], x_ssem.at[4], kv_rsem.at[sp, 2], large_sp, dcore),
    ]
    two_away = (2 * c + 5 - x) % 4 == 2
    relays = x == 2 * c
    through = [
        remote(p[0], rbuf.at[k], p[2], relay_sem.at[k], 4 * z + xu, tp) for k, p in enumerate(kv_puts[2:])
    ]
    onward = [
        remote(rbuf.at[k], kv.at[4 * z + xd, b], relay_sem.at[3 + k], kv_rsem.at[4 * z + xd, b], 4 * z + xu, 2 * y + 1)
        for k, b in enumerate((0, 1, 2))
    ]
    low = jnp.minimum(sp, 15 - sp)
    hi = sp // 8
    qz_at = jnp.where(low < 4, low // 2 + 2, 3 - low // 2)
    qsp = 4 * qz_at + 2 * c
    qtp = 2 * y + low % 2
    q_puts = [
        (qs, qb.at[hi, 0], q_ssem.at[0], q_rsem.at[hi, 0], qsp, qtp),
        (ql.at[:, pl.ds(0, 128)], qb.at[hi, 0], q_ssem.at[1], q_rsem.at[hi, 0], qsp + 1, qtp),
        (ql.at[:, pl.ds(128, 128)], qb.at[hi, 1], q_ssem.at[2], q_rsem.at[hi, 1], qsp + 1, qtp),
        (lam_in.at[0], lam.at[hi], q_ssem.at[3], q_rsem.at[hi, 2], qsp, qtp),
        (lam_in.at[1], lam.at[hi], q_ssem.at[4], q_rsem.at[hi, 2], qsp + 1, qtp),
    ]
    barrier = pltpu.get_barrier_semaphore()

    def greet(dsp, dtp):
        @pl.when(jnp.logical_not(jnp.logical_and(dsp == sp, dtp == tp)))
        def _():
            pl.semaphore_signal(barrier, inc=1, device_id=(dsp, dtp), device_id_type=MESH)

    sources = [(4 * z + c, 2 * y + x // 2), (4 * z + c + 2, 2 * y + x // 2)]
    targets = [(small_sp, dcore), (large_sp, dcore)]
    sources += [(lo_chunk, 2 * y + x // 2), (hi_chunk, 2 * y + x // 2)]
    targets += [(qsp, qtp), (qsp + 1, qtp)]
    near = [(4 * zu + x, tp), (4 * zd + x, tp), (4 * z + xu, tp), (4 * z + xd, tp)]
    near += [(sp, 2 * yu + c), (sp, 2 * yd + c), (sp, 2 * y + 1 - c)]
    sources += near + [(4 * qz_at + a, 2 * b + low % 2) for a in range(4) for b in range(4)]
    targets += near + [(a, t) for a in (lo_chunk, hi_chunk) for t in range(8)]
    for d in sources:
        greet(*d)

    @pl.when(jnp.logical_and(large, c == 1))
    def _():
        greet(4 * z + xd, 2 * y + x // 2)

    count = len(targets) + relays.astype(jnp.int32)
    for d in targets:
        count -= jnp.logical_and(d[0] == sp, d[1] == tp).astype(jnp.int32)
    with jax.named_scope("barrier"):
        pl.semaphore_wait(barrier, count)
    for d in staged:
        d.wait()

    @pl.when(two_away)
    def _():
        for d in through:
            d.start()

    @pl.when(jnp.logical_not(two_away))
    def _():
        for p in kv_puts[2:]:
            put(*p)

    for p in q_puts[1:3] + q_puts[4:] + kv_puts[:2] + q_puts[:1] + q_puts[3:4]:
        put(*p)

    own_piece = (gw, uw, dw.at[pl.ds(0, 352), :], dw.at[pl.ds(352, 352), :])

    def piece(s, k):
        return wt.at[s, k] if k < 2 else wt.at[s, 2, pl.ds(352 * (k - 2), 352), :]

    class Ring:
        def __init__(self, at, along_x, first, line):
            self.at, self.first = at, first
            if along_x:
                self.slots = [4 * line + p for p in (x, xd, xu, x2)]
                self.up, self.down = 4 * z + xu, 4 * z + xd
            else:
                self.slots = [4 * p + line for p in (z, zd, zu, z2)]
                self.up, self.down = 4 * zu + x, 4 * zd + x

        def send(self, n, which, k, to, src=None):
            s = self.slots[which]
            ref = piece(s, k)
            return remote(ref if src is None else src, ref, g_ssem.at[self.at, n], g_rsem.at[s, k], to, tp)

        def own_sends(self, from_input=False):
            a, b = self.first, self.first + 1
            sa, sb = (own_piece[a], own_piece[b]) if from_input else (None, None)
            return [
                self.send(0, 0, a, self.up, sa), self.send(1, 0, b, self.down, sb),
                self.send(2, 0, b, self.up, sb), self.send(3, 0, a, self.down, sa),
            ]

        def far_sends(self):
            return self.send(4, 1, self.first, self.up), self.send(5, 2, self.first + 1, self.down)

        def got(self, which, k):
            got(piece(self.slots[which], k), g_rsem.at[self.slots[which], k])

        def own(self, from_input=False):
            for d in self.own_sends(from_input):
                d.start()

        def forward(self):
            f1, f2 = self.far_sends()
            self.got(1, self.first)
            f1.start()
            self.got(2, self.first + 1)
            f2.start()

        def first_far(self):
            self.got(1, self.first)
            self.got(2, self.first + 1)

        def near(self):
            self.got(1, self.first + 1)
            self.got(2, self.first)

        def far(self):
            self.got(3, self.first)
            self.got(3, self.first + 1)

        def drain(self):
            for d in (*self.own_sends(), *self.far_sends()):
                d.wait_send()

    r0 = Ring(0, False, 0, x)
    r1, r2, r3, r4 = [Ring(1 + n, True, 0, line) for n, line in enumerate((z, zd, zu, z2))]
    r5 = Ring(5, True, 2, z)
    r6, r7, r8, r9 = [Ring(6 + n, False, 2, line) for n, line in enumerate((x, xd, xu, x2))]
    r0.own(True)

    @pl.when(relays)
    def _():
        for k, d in enumerate(onward):
            got(rbuf.at[k], relay_sem.at[k])
            d.start()


    wu, wd = 2 * yu + c, 2 * yd + c
    partner = 2 * y + 1 - c

    def w_send(slot, ssem, dtp, src=None):
        ref = wo.at[slot]
        return remote(ref if src is None else src, ref, ssem, w_rsem.at[slot], sp, dtp)

    own_a, own_b = tp, 8 + tp
    w_own = [
        w_send(own_a, wu_ssem.at[0], wu, osm), w_send(own_b, wd_ssem.at[0], wd, ola),
        w_send(own_b, wu_ssem.at[1], wu, ola), w_send(own_a, wd_ssem.at[1], wd, osm),
        w_send(own_a, wp_ssem.at[0], partner, osm), w_send(own_b, wp_ssem.at[1], partner, ola),
    ]
    for d in w_own:
        d.start()
    pltpu.make_async_copy(osm, wo.at[own_a], l_sem.at[0]).start()
    pltpu.make_async_copy(ola, wo.at[own_b], l_sem.at[1]).start()
    fwd_a, fwd_b = wd, 8 + wu
    w_f1 = [
        (fwd_a, w_send(fwd_a, wu_ssem.at[2], wu), w_send(fwd_a, wp_ssem.at[2], partner)),
        (fwd_b, w_send(fwd_b, wd_ssem.at[2], wd), w_send(fwd_b, wp_ssem.at[3], partner)),
    ]
    w_f2 = [
        (8 + wd, w_send(8 + wd, wp_ssem.at[4], partner)),
        (wu, w_send(wu, wp_ssem.at[5], partner)),
    ]
    w2 = 2 * y2 + c
    w_f3 = [
        (w2, w_send(w2, wp_ssem.at[6], partner)),
        (8 + w2, w_send(8 + w2, wp_ssem.at[7], partner)),
    ]

    def w_forward(items):
        for item in items:
            got(wo.at[item[0]], w_rsem.at[item[0]])
            for d in item[1:]:
                d.start()

    for n, a in enumerate((gw, uw, dw)):
        pltpu.make_async_copy(a, wt.at[sp, n], i_sem.at[6 + n]).start()
    acc[...] = jnp.zeros_like(acc)
    mx[...] = jnp.full_like(mx, masked_score)

    factor = jnp.where(large, log2e * 128**-0.5, log2e * 64**-0.5).astype(F32)
    half = CH // 2

    def absorb(h, first, shift):
        subs = [(m, t) for m in range(2) for t in range(2)]
        values = jnp.concatenate(
            [jnp.concatenate([kv[first + a, 1], jnp.ones((CH, 128), BF)], axis=1) for a in range(2)], axis=0
        )

        def scores(m, t):
            found = []
            for a in range(2):
                s = lax.dot_general(
                    qz[h, m, pl.ds(t * half, half), :], kv[first + a, 2 * m * kind],
                    (((1,), (1,)), ((), ())), preferred_element_type=F32,
                )
                if shift is not None:
                    qi = lax.broadcasted_iota(jnp.int32, (half, CH), 0) + (shift + t * half)
                    ki = lax.broadcasted_iota(jnp.int32, (half, CH), 1) + a * CH
                    s = jnp.where(ki <= qi, s, masked_score)
                found.append(s)
            return found, jnp.max(jnp.maximum(found[0], found[1]), axis=1, keepdims=True)

        now = scores(*subs[0])
        for i, (m, t) in enumerate(subs):
            later = scores(*subs[i + 1]) if i < 3 else None
            rows = pl.ds(t * half, half)
            old = mx[h, m, rows, :]
            new = jnp.maximum(old, now[1])
            mx[h, m, rows, :] = new
            wide = jnp.concatenate([new] * 4, axis=1)
            p = jnp.concatenate([jnp.exp2((s - wide) * factor).astype(BF) for s in now[0]], axis=1)
            fade = jnp.exp2((old - new) * factor)
            pv = jnp.dot(p, values, preferred_element_type=F32)
            acc[h, m, rows, 0:128] = acc[h, m, rows, 0:128] * fade + pv[:, 0:128]
            acc[h, m, rows, 128:256] = acc[h, m, rows, 128:256] * fade + pv[:, 128:256]
            now = later

    slot = 8 * kind + 2 * y + x // 2

    def finish(h):
        for t in range(2):
            rows = pl.ds(t * half, half)
            one = acc[h, 0, rows, 0:128] / acc[h, 0, rows, 128:256]
            two = acc[h, 1, rows, 0:128] / acc[h, 1, rows, 128:256]
            combined = one - lam[h, 0:1, :] * two
            square = jnp.mean(combined * combined, axis=1, keepdims=True)
            normed = combined * lax.rsqrt(square + norm_epsilon) * gain[...] * branch_scale
            ob[h, rows, :] = normed.astype(BF)
        dsp = hi_chunk if h == 1 else lo_chunk
        for t in range(8):
            put(ob.at[h, pl.ds(64 * t, 64), :], att.at[slot], o_ssem.at[h, t], o_rsem.at[slot], dsp, t)

    def kv_send(j, slab, ssem, dsp, dtp):
        return remote(kv.at[j, slab], kv.at[j, slab], ssem, kv_rsem.at[j, slab], dsp, dtp)

    def slabs(fn):
        fn(0)
        fn(1)

        @pl.when(large)
        def _():
            fn(2)

    def route(i):
        own = i < 2
        off = jnp.where(own, 0, jnp.where((i == 2) | (i == 4), 3, jnp.where(i < 6, 1, 2)))
        part = jnp.where((i == 0) | (i == 2) | (i == 5) | (i == 6), 0, 1)
        level = (z + off) % 4
        up = own | (i == 2)
        down = own | (i == 3)
        return level, part, up, down

    def kv_moves(i, act):
        level, part, up, down = route(i)
        j = 4 * level + 2 * part + c

        def one(s):
            @pl.when(up)
            def _():
                act(kv_send(j, s, up_ssem.at[jnp.minimum(i, 2), s], 4 * zu + x, tp))

            @pl.when(down)
            def _():
                act(kv_send(j, s, dn_ssem.at[jnp.minimum(i, 2), s], 4 * zd + x, tp))

            act(kv_send(j, s, pr_ssem.at[i, s], sp, partner))

        slabs(one)

    def kv_arrive(i):
        level, part, up, down = route(i)
        mine = 4 * level + 2 * part + c
        with jax.named_scope("wait_kv"):
            slabs(lambda s: got(kv.at[mine, s], kv_rsem.at[mine, s]))
        kv_moves(i, lambda d: d.start())

    kv_arrive(0)
    kv_arrive(1)
    r5.own(True)
    r1.own(True)
    for d in small_in:
        d.wait()
    with jax.named_scope("wait_q"):
        for h in range(2):
            got(qb.at[h, 0], q_rsem.at[h, 0])
            got(lam.at[h], q_rsem.at[h, 2])

            @pl.when(large)
            def _():
                got(qb.at[h, 1], q_rsem.at[h, 1])
                qz[h, 0] = qb[h, 0]
                qz[h, 1] = qb[h, 1]

            @pl.when(jnp.logical_not(large))
            def _():
                both = qb[h, 0]
                first = lax.broadcasted_iota(jnp.int32, (CH, 128), 1) < 64
                qz[h, 0] = jnp.where(first, both, jnp.zeros_like(both))
                qz[h, 1] = jnp.where(first, jnp.zeros_like(both), both)


    def phase(i, carry):
        level, part, up, down = route(i)
        first = 4 * level + 2 * part
        other = first + 1 - c

        @pl.when((i >= 1) & (i < 5))
        def _():
            kv_arrive(i + 1)

        with jax.named_scope("ev_w"):
            @pl.when(i == 1)
            def _():
                r0.first_far()
                r5.forward()
                r0.near()
                r2.own()
                r3.own()

            @pl.when(i == 2)
            def _():
                for d in r0.far_sends():
                    d.start()
                w_forward(w_f1)

            @pl.when(i == 4)
            def _():
                r6.own(True)
                r1.forward()
                w_forward(w_f2)

            @pl.when(i == 6)
            def _():
                @pl.when(z != 2)
                def _():
                    finish(0)

                w_forward(w_f3)

        with jax.named_scope("wait_kv2"):
            slabs(lambda s: got(kv.at[other, s], kv_rsem.at[other, s]))
        n_lo = jnp.where(lo_chunk >= first, 1, 0)
        n_hi = jnp.where(hi_chunk >= first, 1, 0)

        def step(k, cc):
            h = jnp.where(k >= n_lo, 1, 0)
            gap = jnp.where(h == 1, hi_chunk, lo_chunk) - first

            @pl.when(gap < 2)
            def _():
                absorb(h, first, gap * CH)

            @pl.when(gap >= 2)
            def _():
                absorb(h, first, None)

            return cc

        with jax.named_scope("attn"):
            lax.fori_loop(0, n_lo + n_hi, step, 0)

        @pl.when(i == 5)
        def _():
            kv_arrive(6)
            kv_arrive(7)

        return carry

    lax.fori_loop(0, 8, phase, 0)

    @pl.when(z == 2)
    def _():
        finish(0)

    finish(1)
    with jax.named_scope("ev_post"):
        r0.far()
        r4.own()
        r5.near()
        r7.own()
        r8.own()
        r5.far()
        r9.own()
        r2.forward()
        r3.forward()
        r6.forward()
    with jax.named_scope("wait_wo"):
        pltpu.make_async_copy(osm, wo.at[own_a], l_sem.at[0]).wait()
        pltpu.make_async_copy(ola, wo.at[own_b], l_sem.at[1]).wait()
        for yy in (y, yu, yd, y2):
            for off in (0, 8):
                s = 2 * yy + 1 - c + off
                got(wo.at[s], w_rsem.at[s])
    pre[...] = residual_scale * res[...].astype(F32)
    for part in range(2):
        with jax.named_scope("wait_att"):
            for s in range(8 * part, 8 * part + 8):
                got(att.at[s], o_rsem.at[s])
        rows = jnp.concatenate([att[s] for s in range(8 * part, 8 * part + 8)], axis=1)
        for n in range(4):
            cols = pl.ds(512 * n, 512)
            w = wo[8 * part : 8 * part + 8, :, cols].reshape(1024, 512)
            pre[:, cols] += jnp.dot(rows, w, preferred_element_type=F32)

    values = pre[...]
    centered = values - jnp.mean(values, axis=1, keepdims=True)
    variance = jnp.mean(centered * centered, axis=1, keepdims=True)
    normed = (centered * lax.rsqrt(variance + norm_epsilon) * ngain[...]).astype(BF)
    nb[tp, 0] = normed[:, 0:1024]
    nb[tp, 1] = normed[:, 1024:2048]

    def n_send(t, k, ssem, dtp):
        return remote(nb.at[t, k], nb.at[t, k], ssem, n_rsem.at[t, k], sp, dtp)

    n_own = [
        n_send(tp, 0, nu_ssem.at[0], wu), n_send(tp, 1, nd_ssem.at[0], wd),
        n_send(tp, 1, nu_ssem.at[1], wu), n_send(tp, 0, nd_ssem.at[1], wd),
        n_send(tp, 0, np_ssem.at[0], partner), n_send(tp, 1, np_ssem.at[1], partner),
    ]
    n_fwd = [
        (wd, 0, [n_send(wd, 0, nu_ssem.at[2], wu), n_send(wd, 0, np_ssem.at[2], partner)]),
        (wu, 1, [n_send(wu, 1, nd_ssem.at[2], wd), n_send(wu, 1, np_ssem.at[3], partner)]),
        (wd, 1, [n_send(wd, 1, np_ssem.at[4], partner)]),
        (wu, 0, [n_send(wu, 0, np_ssem.at[5], partner)]),
        (w2, 0, [n_send(w2, 0, np_ssem.at[6], partner)]),
        (w2, 1, [n_send(w2, 1, np_ssem.at[7], partner)]),
    ]
    for d in n_own:
        d.start()
    def n_forward(items):
        for t, k, sends in items:
            got(nb.at[t, k], n_rsem.at[t, k])
            for d in sends:
                d.start()

    with jax.named_scope("ev_post2"):
        r7.forward()
        r8.forward()
        r4.forward()
    with jax.named_scope("wait_nb0"):
        n_forward(n_fwd[:2])
    with jax.named_scope("ev_post3"):
        r9.forward()
    with jax.named_scope("wait_nb"):
        n_forward(n_fwd[2:])
    for n, a in enumerate((gw, uw, dw)):
        pltpu.make_async_copy(a, wt.at[sp, n], i_sem.at[6 + n]).wait()
    with jax.named_scope("wait_w"):
        for ring in (r1, r2, r3, r4, r6, r7, r8, r9):
            ring.near()
            ring.far()

    def mixer(groups):
        rows = []
        for g, yy in groups:
            t = 2 * yy + 1 - c
            got(nb.at[t, 0], n_rsem.at[t, 0])
            got(nb.at[t, 1], n_rsem.at[t, 1])
            for t in (2 * yy + 1 - c, 2 * yy + c):
                rows.append(jnp.concatenate([nb[t, 0], nb[t, 1]], axis=1))
        rows = jnp.concatenate(rows, axis=0)
        nt = (((1,), (1,)), ((), ()))
        gate = lax.dot_general(
            rows, jnp.concatenate([wt[s, 0] for s in range(16)], axis=1), nt, preferred_element_type=F32
        )
        up = lax.dot_general(
            rows, jnp.concatenate([wt[s, 1] for s in range(16)], axis=1), nt, preferred_element_type=F32
        )
        hidden = (gate / (1.0 + jnp.exp(-gate)) * up).astype(BF)
        for n in range(8):
            cols = pl.ds(256 * n, 256)
            w = jnp.concatenate([wt[2 * n, 2], wt[2 * n + 1, 2]], axis=1)
            part = jnp.dot(hidden, w, preferred_element_type=F32)
            for at, (g, yy) in enumerate(groups):
                psend[g, :, cols] = part[128 * at : 128 * at + 64].astype(BF)
                mine_f[g, :, cols] = part[128 * at + 64 : 128 * at + 128]
        for g, yy in groups:
            p_move(g).start()

    def p_move(g):
        return remote(psend.at[g], precv.at[g], p_ssem.at[g], p_rsem.at[g], sp, partner)

    def pair_sum(g, k):
        cols = pl.ds(1024 * k, 1024)
        return mine_f[g, :, cols] + precv[g, :, cols].astype(F32)

    r_a = remote(rsend.at[0, 0], tbuf.at[0], r_ssem.at[0], t_rsem.at[0], sp, wu)
    r_b = remote(rsend.at[0, 1], tbuf.at[1], r_ssem.at[1], t_rsem.at[1], sp, wd)
    up_a = remote(rsend.at[1, 0], rrecv.at[0, 0], r_ssem.at[2], r_rsem.at[0], sp, wu)
    up_b = remote(rsend.at[1, 1], rrecv.at[0, 1], r_ssem.at[3], r_rsem.at[1], sp, wu)
    down_a = remote(rsend.at[2, 0], rrecv.at[1, 0], r_ssem.at[4], r_rsem.at[2], sp, wd)
    down_b = remote(rsend.at[2, 1], rrecv.at[1, 1], r_ssem.at[5], r_rsem.at[3], sp, wd)
    with jax.named_scope("mix0"):
        mixer([(0, y2)])
    with jax.named_scope("pair0"):
        got(precv.at[0], p_rsem.at[0])
        rsend[0, 0] = pair_sum(0, 0).astype(BF)
        r_a.start()
        rsend[0, 1] = pair_sum(0, 1).astype(BF)
        r_b.start()
    with jax.named_scope("mix1"):
        mixer([(1, yu), (2, yd)])
    with jax.named_scope("pair12"):
        got(precv.at[1], p_rsem.at[1])
        rsend[1, 1] = pair_sum(1, 1).astype(BF)
        up_b.start()
        got(precv.at[2], p_rsem.at[2])
        rsend[2, 0] = pair_sum(2, 0).astype(BF)
        down_a.start()
        got(tbuf.at[0], t_rsem.at[0])
        rsend[1, 0] = (pair_sum(1, 0) + tbuf[0].astype(F32)).astype(BF)
        up_a.start()
        got(tbuf.at[1], t_rsem.at[1])
        rsend[2, 1] = (pair_sum(2, 1) + tbuf[1].astype(F32)).astype(BF)
        down_b.start()
    with jax.named_scope("mix3"):
        mixer([(3, y)])
    got(precv.at[3], p_rsem.at[3])
    pre[...] = residual_scale * normed.astype(F32) + 0.5 * (mine_f[3] + precv[3].astype(F32))
    with jax.named_scope("wait_r"):
        for k in range(2):
            got(rrecv.at[0, k], r_rsem.at[k])
            got(rrecv.at[1, k], r_rsem.at[2 + k])
    for k in range(2):
        cols = pl.ds(1024 * k, 1024)
        more = rrecv[0, k].astype(F32) + rrecv[1, k].astype(F32)
        out[:, cols] = (pre[:, cols] + 0.5 * more).astype(BF)

    @pl.when(two_away)
    def _():
        for d in through:
            d.wait_send()

    @pl.when(jnp.logical_not(two_away))
    def _():
        for p in kv_puts[2:]:
            put_done(*p)

    @pl.when(relays)
    def _():
        for d in onward:
            d.wait_send()

    for p in kv_puts[:2]:
        put_done(*p)
    for p in q_puts:
        put_done(*p)
    for d in w_own:
        d.wait_send()
    for item in w_f1 + w_f2 + w_f3:
        for d in item[1:]:
            d.wait_send()

    for ring in (r0, r1, r2, r3, r4, r5, r6, r7, r8, r9):
        ring.drain()
    for d in n_own:
        d.wait_send()
    for t, k, sends in n_fwd:
        for d in sends:
            d.wait_send()
    for g in range(4):
        p_move(g).wait_send()
    for d in (r_a, r_b, up_a, up_b, down_a, down_b):
        d.wait_send()

    def drain(i, carry):
        kv_moves(i, lambda d: d.wait_send())
        return carry

    lax.fori_loop(0, 8, drain, 0)
    for h in range(2):
        dsp = hi_chunk if h == 1 else lo_chunk
        for t in range(8):
            put_done(ob.at[h, pl.ds(64 * t, 64), :], att.at[slot], o_ssem.at[h, t], o_rsem.at[slot], dsp, t)


def block(*args):
    dma = pltpu.SemaphoreType.DMA
    return pl.pallas_call(
        block_kernel,
        name="block",
        out_shape=pltpu.VMEM((64, 2048), BF),
        in_specs=[
            pl.BlockSpec(memory_space={"h": pl.ANY, "v": pltpu.VMEM, "s": pltpu.SMEM}[k])
            for k in "hhhhhhsshhhhhhhh"
        ],
        out_specs=pl.BlockSpec(memory_space=pltpu.VMEM),
        scratch_shapes=[
            pltpu.VMEM((CH, 128), BF), pltpu.VMEM((CH, 256), BF), pltpu.VMEM((CH, 128), BF),
            pltpu.VMEM((CH, 256), BF), pltpu.VMEM((CH, 128), BF), pltpu.VMEM((CH, 128), BF),
            pltpu.VMEM((2, 8, 128), F32), pltpu.VMEM((1, 128), F32), pltpu.VMEM((64, 2048), BF),
            pltpu.VMEM((1, 2048), F32),
            pltpu.VMEM((16, 3, CH, 128), BF),
            pltpu.VMEM((2, 2, CH, 128), BF),
            pltpu.VMEM((2, 2, CH, 128), BF),
            pltpu.VMEM((2, 8, 128), F32),
            pltpu.VMEM((2, 2, CH, 256), F32),
            pltpu.VMEM((2, 2, CH, 128), F32),
            pltpu.VMEM((16, 128, 2048), BF),
            pltpu.VMEM((2, CH, 128), BF),
            pltpu.VMEM((16, 64, 128), BF),
            pltpu.VMEM((64, 2048), F32),
            pltpu.VMEM((16, 3, 704, 128), BF),
            pltpu.VMEM((8, 2, 64, 1024), BF),
            pltpu.VMEM((4, 64, 2048), BF),
            pltpu.VMEM((4, 64, 2048), BF),
            pltpu.VMEM((4, 64, 2048), F32),
            pltpu.VMEM((3, 2, 64, 1024), BF),
            pltpu.VMEM((2, 2, 64, 1024), BF),
            pltpu.VMEM((2, 64, 1024), BF),
            pltpu.VMEM((3, CH, 128), BF),
            dma((5,)), dma((2, 3)), dma((5,)), dma((16, 3)), dma((3, 3)), dma((3, 3)), dma((8, 3)),
            dma((3,)), dma((3,)), dma((8,)), dma((16,)), dma((2, 8)), dma((16,)), dma((2,)),
            dma((10, 6)), dma((16, 4)), dma((3,)), dma((3,)), dma((8,)), dma((8, 2)),
            dma((4,)), dma((4,)), dma((6,)), dma((4,)), dma((2,)), dma((12,)), dma((6,)),
        ],
        compiler_params=pltpu.CompilerParams(has_side_effects=True, collective_id=0, vmem_limit_bytes=60 * 1024 * 1024),
        cost_estimate=pl.CostEstimate(flops=8 * 10**9, bytes_accessed=10**8, transcendentals=10**7),
    )(*args)


def per_device(
    residual, query_small, key_small, value_small, query_large, key_large, value_large,
    lambda_small, lambda_large, head_gain, output_small, output_large, norm_gain,
    gate_weight, up_weight, down_weight,
):
    flat = lambda a: a.reshape(a.shape[0], a.shape[2])
    return block(
        flat(query_small), flat(query_large), flat(key_small), flat(key_large), flat(value_small),
        flat(value_large), lambda_small, lambda_large, head_gain.reshape(1, 128), output_small, output_large, residual,
        norm_gain.reshape(1, 2048), gate_weight.T, up_weight.T, down_weight,
    )


def solution(mesh):
    in_specs = (
        P(("sp", "tp"), None),
        P("sp", "tp", None), P("sp", "tp", None), P("sp", "tp", None),
        P("sp", "tp", None), P("sp", "tp", None), P("sp", "tp", None),
        P("tp"), P("tp"), P(), P("tp", None), P("tp", None), P(),
        P("sp", "tp"), P("sp", "tp"), P("tp", "sp"),
    )
    return jax.shard_map(
        per_device, mesh=mesh, in_specs=in_specs, out_specs=P(("sp", "tp"), None), check_vma=False
    )
```

```python
import math

import jax
import jax.numpy as jnp
from jax import lax
from jax.experimental import pallas as pl
from jax.experimental.pallas import tpu as pltpu
from jax.sharding import PartitionSpec as P

residual_scale = 8.0**0.25
branch_scale = 0.8
norm_epsilon = 1e-05
masked_score = -1e30
log2e = math.log2(math.e)
MESH = pl.DeviceIdType.MESH
BF = jnp.bfloat16
F32 = jnp.float32
CH = 512


def remote(src, dst, ssem, rsem, sp, tp):
    return pltpu.make_async_remote_copy(
        src_ref=src, dst_ref=dst, send_sem=ssem, recv_sem=rsem, device_id=(sp, tp), device_id_type=MESH
    )


def block_kernel(
    qs_in, ql_in, ks_in, kl_in, vs_in, vl_in, lam_s, lam_l, gain_in, osm, ola, res_in, ngain_in, gw, uw, dw,
    out,
    qs, ql, ks, kl, vs, vl, lam_in, gain, res, ngain, kv, qb, qz, lam, acc, mx, wo, ob, att, pre, wt, nb, psend, precv, mine_f, rsend, rrecv, tbuf, rbuf,
    q_ssem, q_rsem, x_ssem, kv_rsem, up_ssem, dn_ssem, pr_ssem,
    wu_ssem, wd_ssem, wp_ssem, w_rsem, o_ssem, o_rsem, l_sem,
    g_ssem, g_rsem, nu_ssem, nd_ssem, np_ssem, n_rsem, p_ssem, p_rsem, r_ssem, r_rsem, t_rsem, i_sem, relay_sem,
):
    sp, tp = lax.axis_index("sp"), lax.axis_index("tp")
    z, x, y, c = sp // 4, sp % 4, tp // 2, tp % 2
    kind = x % 2
    large = kind == 1
    zu, zd, z2 = (z + 1) % 4, (z + 3) % 4, (z + 2) % 4
    yu, yd, y2 = (y + 1) % 4, (y + 3) % 4, (y + 2) % 4
    xu, xd, x2 = (x + 1) % 4, (x + 3) % 4, (x + 2) % 4
    r = 2 * jnp.where(z < 2, 3 - z, z - 2) + c
    lo_chunk, hi_chunk = r, 15 - r

    def put(src, dst, ssem, rsem, dsp, dtp):
        same = jnp.logical_and(dsp == sp, dtp == tp)

        @pl.when(same)
        def _():
            pltpu.make_async_copy(src, dst, rsem).start()

        @pl.when(jnp.logical_not(same))
        def _():
            remote(src, dst, ssem, rsem, dsp, dtp).start()

    def put_done(src, dst, ssem, rsem, dsp, dtp):
        same = jnp.logical_and(dsp == sp, dtp == tp)

        @pl.when(jnp.logical_not(same))
        def _():
            remote(src, dst, ssem, rsem, dsp, dtp).wait_send()

    def got(dst, rsem):
        pltpu.make_async_copy(dst, dst, rsem).wait()

    staged = [
        pltpu.make_async_copy(a, b, i_sem.at[n])
        for n, (a, b) in enumerate(
            ((ks_in, ks), (vs_in, vs), (kl_in, kl), (vl_in, vl), (qs_in, qs), (ql_in, ql))
        )
    ]
    for d in staged:
        d.start()
    small_in = [
        pltpu.make_async_copy(a, b, i_sem.at[9 + n])
        for n, (a, b) in enumerate(((gain_in, gain), (res_in, res), (ngain_in, ngain)))
    ]
    for d in small_in:
        d.start()
    lam_in[0] = jnp.full((8, 128), lam_s[0], F32)
    lam_in[1] = jnp.full((8, 128), lam_l[0], F32)
    dcore = 2 * y + x % 2
    small_sp, large_sp = 4 * z + 2 * c, 4 * z + 2 * c + 1
    kv_puts = [
        (ks, kv.at[sp, 0], x_ssem.at[0], kv_rsem.at[sp, 0], small_sp, dcore),
        (vs, kv.at[sp, 1], x_ssem.at[1], kv_rsem.at[sp, 1], small_sp, dcore),
        (kl.at[:, pl.ds(0, 128)], kv.at[sp, 0], x_ssem.at[2], kv_rsem.at[sp, 0], large_sp, dcore),
        (vl, kv.at[sp, 1], x_ssem.at[3], kv_rsem.at[sp, 1], large_sp, dcore),
        (kl.at[:, pl.ds(128, 128)], kv.at[sp, 2], x_ssem.at[4], kv_rsem.at[sp, 2], large_sp, dcore),
    ]
    two_away = (2 * c + 5 - x) % 4 == 2
    relays = x == 2 * c
    through = [
        remote(p[0], rbuf.at[k], p[2], relay_sem.at[k], 4 * z + xu, tp) for k, p in enumerate(kv_puts[2:])
    ]
    onward = [
        remote(rbuf.at[k], kv.at[4 * z + xd, b], relay_sem.at[3 + k], kv_rsem.at[4 * z + xd, b], 4 * z + xu, 2 * y + 1)
        for k, b in enumerate((0, 1, 2))
    ]
    low = jnp.minimum(sp, 15 - sp)
    hi = sp // 8
    qz_at = jnp.where(low < 4, low // 2 + 2, 3 - low // 2)
    qsp = 4 * qz_at + 2 * c
    qtp = 2 * y + low % 2
    q_puts = [
        (qs, qb.at[hi, 0], q_ssem.at[0], q_rsem.at[hi, 0], qsp, qtp),
        (ql.at[:, pl.ds(0, 128)], qb.at[hi, 0], q_ssem.at[1], q_rsem.at[hi, 0], qsp + 1, qtp),
        (ql.at[:, pl.ds(128, 128)], qb.at[hi, 1], q_ssem.at[2], q_rsem.at[hi, 1], qsp + 1, qtp),
        (lam_in.at[0], lam.at[hi], q_ssem.at[3], q_rsem.at[hi, 2], qsp, qtp),
        (lam_in.at[1], lam.at[hi], q_ssem.at[4], q_rsem.at[hi, 2], qsp + 1, qtp),
    ]
    barrier = pltpu.get_barrier_semaphore()

    def greet(dsp, dtp):
        @pl.when(jnp.logical_not(jnp.logical_and(dsp == sp, dtp == tp)))
        def _():
            pl.semaphore_signal(barrier, inc=1, device_id=(dsp, dtp), device_id_type=MESH)

    sources = [(4 * z + c, 2 * y + x // 2), (4 * z + c + 2, 2 * y + x // 2)]
    targets = [(small_sp, dcore), (large_sp, dcore)]
    sources += [(lo_chunk, 2 * y + x // 2), (hi_chunk, 2 * y + x // 2)]
    targets += [(qsp, qtp), (qsp + 1, qtp)]
    near = [(4 * zu + x, tp), (4 * zd + x, tp), (4 * z + xu, tp), (4 * z + xd, tp)]
    near += [(sp, 2 * yu + c), (sp, 2 * yd + c), (sp, 2 * y + 1 - c)]
    sources += near + [(4 * qz_at + a, 2 * b + low % 2) for a in range(4) for b in range(4)]
    targets += near + [(a, t) for a in (lo_chunk, hi_chunk) for t in range(8)]
    for d in sources:
        greet(*d)

    @pl.when(jnp.logical_and(large, c == 1))
    def _():
        greet(4 * z + xd, 2 * y + x // 2)

    count = len(targets) + relays.astype(jnp.int32)
    for d in targets:
        count -= jnp.logical_and(d[0] == sp, d[1] == tp).astype(jnp.int32)
    with jax.named_scope("barrier"):
        pl.semaphore_wait(barrier, count)
    for d in staged:
        d.wait()

    @pl.when(two_away)
    def _():
        for d in through:
            d.start()

    @pl.when(jnp.logical_not(two_away))
    def _():
        for p in kv_puts[2:]:
            put(*p)

    for p in q_puts[1:3] + q_puts[4:] + kv_puts[:2] + q_puts[:1] + q_puts[3:4]:
        put(*p)

    own_piece = (gw, uw, dw.at[pl.ds(0, 352), :], dw.at[pl.ds(352, 352), :])

    def piece(s, k):
        return wt.at[s, k] if k < 2 else wt.at[s, 2, pl.ds(352 * (k - 2), 352), :]

    class Ring:
        def __init__(self, at, along_x, first, line):
            self.at, self.first = at, first
            if along_x:
                self.slots = [4 * line + p for p in (x, xd, xu, x2)]
                self.up, self.down = 4 * z + xu, 4 * z + xd
            else:
                self.slots = [4 * p + line for p in (z, zd, zu, z2)]
                self.up, self.down = 4 * zu + x, 4 * zd + x

        def send(self, n, which, k, to, src=None):
            s = self.slots[which]
            ref = piece(s, k)
            return remote(ref if src is None else src, ref, g_ssem.at[self.at, n], g_rsem.at[s, k], to, tp)

        def own_sends(self, from_input=False):
            a, b = self.first, self.first + 1
            sa, sb = (own_piece[a], own_piece[b]) if from_input else (None, None)
            return [
                self.send(0, 0, a, self.up, sa), self.send(1, 0, b, self.down, sb),
                self.send(2, 0, b, self.up, sb), self.send(3, 0, a, self.down, sa),
            ]

        def far_sends(self):
            return self.send(4, 1, self.first, self.up), self.send(5, 2, self.first + 1, self.down)

        def got(self, which, k):
            got(piece(self.slots[which], k), g_rsem.at[self.slots[which], k])

        def own(self, from_input=False):
            for d in self.own_sends(from_input):
                d.start()

        def forward(self):
            f1, f2 = self.far_sends()
            self.got(1, self.first)
            f1.start()
            self.got(2, self.first + 1)
            f2.start()

        def first_far(self):
            self.got(1, self.first)
            self.got(2, self.first + 1)

        def near(self):
            self.got(1, self.first + 1)
            self.got(2, self.first)

        def far(self):
            self.got(3, self.first)
            self.got(3, self.first + 1)

        def drain(self):
            for d in (*self.own_sends(), *self.far_sends()):
                d.wait_send()

    r0 = Ring(0, False, 0, x)
    r1, r2, r3, r4 = [Ring(1 + n, True, 0, line) for n, line in enumerate((z, zd, zu, z2))]
    r5 = Ring(5, True, 2, z)
    r6, r7, r8, r9 = [Ring(6 + n, False, 2, line) for n, line in enumerate((x, xd, xu, x2))]
    r0.own(True)

    @pl.when(relays)
    def _():
        for k, d in enumerate(onward):
            got(rbuf.at[k], relay_sem.at[k])
            d.start()


    wu, wd = 2 * yu + c, 2 * yd + c
    partner = 2 * y + 1 - c

    def w_send(slot, ssem, dtp, src=None):
        ref = wo.at[slot]
        return remote(ref if src is None else src, ref, ssem, w_rsem.at[slot], sp, dtp)

    own_a, own_b = tp, 8 + tp
    w_own = [
        w_send(own_a, wu_ssem.at[0], wu, osm), w_send(own_b, wd_ssem.at[0], wd, ola),
        w_send(own_b, wu_ssem.at[1], wu, ola), w_send(own_a, wd_ssem.at[1], wd, osm),
        w_send(own_a, wp_ssem.at[0], partner, osm), w_send(own_b, wp_ssem.at[1], partner, ola),
    ]
    for d in w_own:
        d.start()
    pltpu.make_async_copy(osm, wo.at[own_a], l_sem.at[0]).start()
    pltpu.make_async_copy(ola, wo.at[own_b], l_sem.at[1]).start()
    fwd_a, fwd_b = wd, 8 + wu
    w_f1 = [
        (fwd_a, w_send(fwd_a, wu_ssem.at[2], wu), w_send(fwd_a, wp_ssem.at[2], partner)),
        (fwd_b, w_send(fwd_b, wd_ssem.at[2], wd), w_send(fwd_b, wp_ssem.at[3], partner)),
    ]
    w_f2 = [
        (8 + wd, w_send(8 + wd, wp_ssem.at[4], partner)),
        (wu, w_send(wu, wp_ssem.at[5], partner)),
    ]
    w2 = 2 * y2 + c
    w_f3 = [
        (w2, w_send(w2, wp_ssem.at[6], partner)),
        (8 + w2, w_send(8 + w2, wp_ssem.at[7], partner)),
    ]

    def w_forward(items):
        for item in items:
            got(wo.at[item[0]], w_rsem.at[item[0]])
            for d in item[1:]:
                d.start()

    for n, a in enumerate((gw, uw, dw)):
        pltpu.make_async_copy(a, wt.at[sp, n], i_sem.at[6 + n]).start()
    acc[...] = jnp.zeros_like(acc)
    mx[...] = jnp.full_like(mx, masked_score)

    factor = jnp.where(large, log2e * 128**-0.5, log2e * 64**-0.5).astype(F32)
    half = CH // 2

    def absorb(h, first, shift):
        subs = [(m, t) for m in range(2) for t in range(2)]
        values = jnp.concatenate(
            [jnp.concatenate([kv[first + a, 1], jnp.ones((CH, 128), BF)], axis=1) for a in range(2)], axis=0
        )

        def scores(m, t):
            found = []
            for a in range(2):
                s = lax.dot_general(
                    qz[h, m, pl.ds(t * half, half), :], kv[first + a, 2 * m * kind],
                    (((1,), (1,)), ((), ())), preferred_element_type=F32,
                )
                if shift is not None:
                    qi = lax.broadcasted_iota(jnp.int32, (half, CH), 0) + (shift + t * half)
                    ki = lax.broadcasted_iota(jnp.int32, (half, CH), 1) + a * CH
                    s = jnp.where(ki <= qi, s, masked_score)
                found.append(s)
            return found, jnp.max(jnp.maximum(found[0], found[1]), axis=1, keepdims=True)

        now = scores(*subs[0])
        for i, (m, t) in enumerate(subs):
            later = scores(*subs[i + 1]) if i < 3 else None
            rows = pl.ds(t * half, half)
            old = mx[h, m, rows, :]
            new = jnp.maximum(old, now[1])
            mx[h, m, rows, :] = new
            wide = jnp.concatenate([new] * 4, axis=1)
            p = jnp.concatenate([jnp.exp2((s - wide) * factor).astype(BF) for s in now[0]], axis=1)
            fade = jnp.exp2((old - new) * factor)
            pv = jnp.dot(p, values, preferred_element_type=F32)
            acc[h, m, rows, 0:128] = acc[h, m, rows, 0:128] * fade + pv[:, 0:128]
            acc[h, m, rows, 128:256] = acc[h, m, rows, 128:256] * fade + pv[:, 128:256]
            now = later

    slot = 8 * kind + 2 * y + x // 2

    def finish(h):
        for t in range(2):
            rows = pl.ds(t * half, half)
            one = acc[h, 0, rows, 0:128] / acc[h, 0, rows, 128:256]
            two = acc[h, 1, rows, 0:128] / acc[h, 1, rows, 128:256]
            combined = one - lam[h, 0:1, :] * two
            square = jnp.mean(combined * combined, axis=1, keepdims=True)
            normed = combined * lax.rsqrt(square + norm_epsilon) * gain[...] * branch_scale
            ob[h, rows, :] = normed.astype(BF)
            dsp = hi_chunk if h == 1 else lo_chunk
            for n in range(4 * t, 4 * t + 4):
                put(ob.at[h, pl.ds(64 * n, 64), :], att.at[slot], o_ssem.at[h, n], o_rsem.at[slot], dsp, n)

    def kv_send(j, slab, ssem, dsp, dtp):
        return remote(kv.at[j, slab], kv.at[j, slab], ssem, kv_rsem.at[j, slab], dsp, dtp)

    def slabs(fn):
        fn(0)
        fn(1)

        @pl.when(large)
        def _():
            fn(2)

    def route(i):
        own = i < 2
        off = jnp.where(own, 0, jnp.where((i == 2) | (i == 4), 3, jnp.where(i < 6, 1, 2)))
        part = jnp.where((i == 0) | (i == 2) | (i == 5) | (i == 6), 0, 1)
        level = (z + off) % 4
        up = own | (i == 2)
        down = own | (i == 3)
        return level, part, up, down

    def kv_moves(i, act):
        level, part, up, down = route(i)
        j = 4 * level + 2 * part + c

        def one(s):
            @pl.when(up)
            def _():
                act(kv_send(j, s, up_ssem.at[jnp.minimum(i, 2), s], 4 * zu + x, tp))

            @pl.when(down)
            def _():
                act(kv_send(j, s, dn_ssem.at[jnp.minimum(i, 2), s], 4 * zd + x, tp))

            act(kv_send(j, s, pr_ssem.at[i, s], sp, partner))

        slabs(one)

    def kv_arrive(i):
        level, part, up, down = route(i)
        mine = 4 * level + 2 * part + c
        with jax.named_scope("wait_kv"):
            slabs(lambda s: got(kv.at[mine, s], kv_rsem.at[mine, s]))
        kv_moves(i, lambda d: d.start())

    kv_arrive(0)
    kv_arrive(1)
    r5.own(True)
    r1.own(True)
    for d in small_in:
        d.wait()
    with jax.named_scope("wait_q"):
        for h in range(2):
            got(qb.at[h, 0], q_rsem.at[h, 0])
            got(lam.at[h], q_rsem.at[h, 2])

            @pl.when(large)
            def _():
                got(qb.at[h, 1], q_rsem.at[h, 1])
                qz[h, 0] = qb[h, 0]
                qz[h, 1] = qb[h, 1]

            @pl.when(jnp.logical_not(large))
            def _():
                both = qb[h, 0]
                first = lax.broadcasted_iota(jnp.int32, (CH, 128), 1) < 64
                qz[h, 0] = jnp.where(first, both, jnp.zeros_like(both))
                qz[h, 1] = jnp.where(first, jnp.zeros_like(both), both)


    def phase(i, carry):
        level, part, up, down = route(i)
        first = 4 * level + 2 * part
        other = first + 1 - c

        @pl.when((i >= 1) & (i < 5))
        def _():
            kv_arrive(i + 1)

        with jax.named_scope("ev_w"):
            @pl.when(i == 1)
            def _():
                r0.first_far()
                r5.forward()
                r0.near()
                r2.own()
                r3.own()

            @pl.when(i == 2)
            def _():
                for d in r0.far_sends():
                    d.start()
                w_forward(w_f1)

            @pl.when(i == 4)
            def _():
                r6.own(True)
                r1.forward()
                w_forward(w_f2)

            @pl.when(i == 6)
            def _():
                @pl.when(z != 2)
                def _():
                    finish(0)

                w_forward(w_f3)

        with jax.named_scope("wait_kv2"):
            slabs(lambda s: got(kv.at[other, s], kv_rsem.at[other, s]))
        n_lo = jnp.where(lo_chunk >= first, 1, 0)
        n_hi = jnp.where(hi_chunk >= first, 1, 0)

        def step(k, cc):
            h = jnp.where(k >= n_lo, 1, 0)
            gap = jnp.where(h == 1, hi_chunk, lo_chunk) - first

            @pl.when(gap < 2)
            def _():
                absorb(h, first, gap * CH)

            @pl.when(gap >= 2)
            def _():
                absorb(h, first, None)

            return cc

        with jax.named_scope("attn"):
            lax.fori_loop(0, n_lo + n_hi, step, 0)

        @pl.when(i == 5)
        def _():
            kv_arrive(6)
            kv_arrive(7)

        return carry

    lax.fori_loop(0, 8, phase, 0)

    @pl.when(z == 2)
    def _():
        finish(0)

    finish(1)
    with jax.named_scope("ev_post"):
        r0.far()
        r4.own()
        r5.near()
        r7.own()
        r8.own()
        r5.far()
        r9.own()
        r2.forward()
        r3.forward()
        r6.forward()
    with jax.named_scope("wait_wo"):
        pltpu.make_async_copy(osm, wo.at[own_a], l_sem.at[0]).wait()
        pltpu.make_async_copy(ola, wo.at[own_b], l_sem.at[1]).wait()
        for yy in (y, yu, yd, y2):
            for off in (0, 8):
                s = 2 * yy + 1 - c + off
                got(wo.at[s], w_rsem.at[s])
    pre[...] = residual_scale * res[...].astype(F32)
    for part in range(2):
        with jax.named_scope("wait_att"):
            for s in range(8 * part, 8 * part + 8):
                got(att.at[s], o_rsem.at[s])
        rows = jnp.concatenate([att[s] for s in range(8 * part, 8 * part + 8)], axis=1)
        for n in range(4):
            cols = pl.ds(512 * n, 512)
            w = wo[8 * part : 8 * part + 8, :, cols].reshape(1024, 512)
            pre[:, cols] += jnp.dot(rows, w, preferred_element_type=F32)

    values = pre[...]
    centered = values - jnp.mean(values, axis=1, keepdims=True)
    variance = jnp.mean(centered * centered, axis=1, keepdims=True)
    normed = (centered * lax.rsqrt(variance + norm_epsilon) * ngain[...]).astype(BF)
    nb[tp, 0] = normed[:, 0:1024]
    nb[tp, 1] = normed[:, 1024:2048]

    def n_send(t, k, ssem, dtp):
        return remote(nb.at[t, k], nb.at[t, k], ssem, n_rsem.at[t, k], sp, dtp)

    n_own = [
        n_send(tp, 0, nu_ssem.at[0], wu), n_send(tp, 1, nd_ssem.at[0], wd),
        n_send(tp, 1, nu_ssem.at[1], wu), n_send(tp, 0, nd_ssem.at[1], wd),
        n_send(tp, 0, np_ssem.at[0], partner), n_send(tp, 1, np_ssem.at[1], partner),
    ]
    n_fwd = [
        (wd, 0, [n_send(wd, 0, nu_ssem.at[2], wu), n_send(wd, 0, np_ssem.at[2], partner)]),
        (wu, 1, [n_send(wu, 1, nd_ssem.at[2], wd), n_send(wu, 1, np_ssem.at[3], partner)]),
        (wd, 1, [n_send(wd, 1, np_ssem.at[4], partner)]),
        (wu, 0, [n_send(wu, 0, np_ssem.at[5], partner)]),
        (w2, 0, [n_send(w2, 0, np_ssem.at[6], partner)]),
        (w2, 1, [n_send(w2, 1, np_ssem.at[7], partner)]),
    ]
    for d in n_own:
        d.start()
    def n_forward(items):
        for t, k, sends in items:
            got(nb.at[t, k], n_rsem.at[t, k])
            for d in sends:
                d.start()

    with jax.named_scope("ev_post2"):
        r7.forward()
        r8.forward()
        r4.forward()
    with jax.named_scope("wait_nb0"):
        n_forward(n_fwd[:2])
    with jax.named_scope("ev_post3"):
        r9.forward()
    with jax.named_scope("wait_nb"):
        n_forward(n_fwd[2:])
    for n, a in enumerate((gw, uw, dw)):
        pltpu.make_async_copy(a, wt.at[sp, n], i_sem.at[6 + n]).wait()
    with jax.named_scope("wait_w"):
        for ring in (r1, r2, r3, r4, r6, r7, r8, r9):
            ring.near()
            ring.far()

    def mixer(groups, between=None):
        rows = []
        for g, yy in groups:
            t = 2 * yy + 1 - c
            got(nb.at[t, 0], n_rsem.at[t, 0])
            got(nb.at[t, 1], n_rsem.at[t, 1])
            for t in (2 * yy + 1 - c, 2 * yy + c):
                rows.append(jnp.concatenate([nb[t, 0], nb[t, 1]], axis=1))
        rows = jnp.concatenate(rows, axis=0)
        nt = (((1,), (1,)), ((), ()))
        gate = lax.dot_general(
            rows, jnp.concatenate([wt[s, 0] for s in range(16)], axis=1), nt, preferred_element_type=F32
        )
        if between is not None:
            between()
        up = lax.dot_general(
            rows, jnp.concatenate([wt[s, 1] for s in range(16)], axis=1), nt, preferred_element_type=F32
        )
        hidden = (gate / (1.0 + jnp.exp(-gate)) * up).astype(BF)
        for n in range(8):
            cols = pl.ds(256 * n, 256)
            w = jnp.concatenate([wt[2 * n, 2], wt[2 * n + 1, 2]], axis=1)
            part = jnp.dot(hidden, w, preferred_element_type=F32)
            for at, (g, yy) in enumerate(groups):
                psend[g, :, cols] = part[128 * at : 128 * at + 64].astype(BF)
                mine_f[g, :, cols] = part[128 * at + 64 : 128 * at + 128]
        for g, yy in groups:
            p_move(g).start()

    def p_move(g):
        return remote(psend.at[g], precv.at[g], p_ssem.at[g], p_rsem.at[g], sp, partner)

    def pair_sum(g, k):
        cols = pl.ds(1024 * k, 1024)
        return mine_f[g, :, cols] + precv[g, :, cols].astype(F32)

    r_a = remote(rsend.at[0, 0], tbuf.at[0], r_ssem.at[0], t_rsem.at[0], sp, wu)
    r_b = remote(rsend.at[0, 1], tbuf.at[1], r_ssem.at[1], t_rsem.at[1], sp, wd)
    up_a = remote(rsend.at[1, 0], rrecv.at[0, 0], r_ssem.at[2], r_rsem.at[0], sp, wu)
    up_b = remote(rsend.at[1, 1], rrecv.at[0, 1], r_ssem.at[3], r_rsem.at[1], sp, wu)
    down_a = remote(rsend.at[2, 0], rrecv.at[1, 0], r_ssem.at[4], r_rsem.at[2], sp, wd)
    down_b = remote(rsend.at[2, 1], rrecv.at[1, 1], r_ssem.at[5], r_rsem.at[3], sp, wd)
    with jax.named_scope("mix0"):
        mixer([(0, y2)])
    def pass_far():
        with jax.named_scope("pair0"):
            got(precv.at[0], p_rsem.at[0])
            rsend[0, 0] = pair_sum(0, 0).astype(BF)
            r_a.start()
            rsend[0, 1] = pair_sum(0, 1).astype(BF)
            r_b.start()

    def pass_near():
        with jax.named_scope("pair12"):
            got(precv.at[1], p_rsem.at[1])
            rsend[1, 1] = pair_sum(1, 1).astype(BF)
            up_b.start()
            got(precv.at[2], p_rsem.at[2])
            rsend[2, 0] = pair_sum(2, 0).astype(BF)
            down_a.start()
            got(tbuf.at[0], t_rsem.at[0])
            rsend[1, 0] = (pair_sum(1, 0) + tbuf[0].astype(F32)).astype(BF)
            up_a.start()
            got(tbuf.at[1], t_rsem.at[1])
            rsend[2, 1] = (pair_sum(2, 1) + tbuf[1].astype(F32)).astype(BF)
            down_b.start()

    mixer([(1, yu), (2, yd)], pass_far)
    mixer([(3, y)], pass_near)
    got(precv.at[3], p_rsem.at[3])
    pre[...] = residual_scale * normed.astype(F32) + 0.5 * (mine_f[3] + precv[3].astype(F32))
    @pl.when(two_away)
    def _():
        for d in through:
            d.wait_send()

    @pl.when(jnp.logical_not(two_away))
    def _():
        for p in kv_puts[2:]:
            put_done(*p)

    @pl.when(relays)
    def _():
        for d in onward:
            d.wait_send()

    for p in kv_puts[:2]:
        put_done(*p)
    for p in q_puts:
        put_done(*p)
    for d in w_own:
        d.wait_send()
    for item in w_f1 + w_f2 + w_f3:
        for d in item[1:]:
            d.wait_send()

    for ring in (r0, r1, r2, r3, r4, r5, r6, r7, r8, r9):
        ring.drain()
    for d in n_own:
        d.wait_send()
    for t, k, sends in n_fwd:
        for d in sends:
            d.wait_send()
    for g in range(4):
        p_move(g).wait_send()

    def drain(i, carry):
        kv_moves(i, lambda d: d.wait_send())
        return carry

    lax.fori_loop(0, 8, drain, 0)
    for h in range(2):
        dsp = hi_chunk if h == 1 else lo_chunk
        for t in range(8):
            put_done(ob.at[h, pl.ds(64 * t, 64), :], att.at[slot], o_ssem.at[h, t], o_rsem.at[slot], dsp, t)

    with jax.named_scope("wait_r"):
        got(rrecv.at[0, 1], r_rsem.at[1])
        got(rrecv.at[1, 0], r_rsem.at[2])
        pre[:, 1024:2048] += 0.5 * rrecv[0, 1].astype(F32)
        pre[:, 0:1024] += 0.5 * rrecv[1, 0].astype(F32)
        got(rrecv.at[0, 0], r_rsem.at[0])
        out[:, 0:1024] = (pre[:, 0:1024] + 0.5 * rrecv[0, 0].astype(F32)).astype(BF)
        got(rrecv.at[1, 1], r_rsem.at[3])
        out[:, 1024:2048] = (pre[:, 1024:2048] + 0.5 * rrecv[1, 1].astype(F32)).astype(BF)
    for d in (r_a, r_b, up_a, up_b, down_a, down_b):
        d.wait_send()


def block(*args):
    dma = pltpu.SemaphoreType.DMA
    return pl.pallas_call(
        block_kernel,
        name="block",
        out_shape=pltpu.VMEM((64, 2048), BF),
        in_specs=[
            pl.BlockSpec(memory_space={"h": pl.ANY, "v": pltpu.VMEM, "s": pltpu.SMEM}[k])
            for k in "hhhhhhsshhhhhhhh"
        ],
        out_specs=pl.BlockSpec(memory_space=pltpu.VMEM),
        scratch_shapes=[
            pltpu.VMEM((CH, 128), BF), pltpu.VMEM((CH, 256), BF), pltpu.VMEM((CH, 128), BF),
            pltpu.VMEM((CH, 256), BF), pltpu.VMEM((CH, 128), BF), pltpu.VMEM((CH, 128), BF),
            pltpu.VMEM((2, 8, 128), F32), pltpu.VMEM((1, 128), F32), pltpu.VMEM((64, 2048), BF),
            pltpu.VMEM((1, 2048), F32),
            pltpu.VMEM((16, 3, CH, 128), BF),
            pltpu.VMEM((2, 2, CH, 128), BF),
            pltpu.VMEM((2, 2, CH, 128), BF),
            pltpu.VMEM((2, 8, 128), F32),
            pltpu.VMEM((2, 2, CH, 256), F32),
            pltpu.VMEM((2, 2, CH, 128), F32),
            pltpu.VMEM((16, 128, 2048), BF),
            pltpu.VMEM((2, CH, 128), BF),
            pltpu.VMEM((16, 64, 128), BF),
            pltpu.VMEM((64, 2048), F32),
            pltpu.VMEM((16, 3, 704, 128), BF),
            pltpu.VMEM((8, 2, 64, 1024), BF),
            pltpu.VMEM((4, 64, 2048), BF),
            pltpu.VMEM((4, 64, 2048), BF),
            pltpu.VMEM((4, 64, 2048), F32),
            pltpu.VMEM((3, 2, 64, 1024), BF),
            pltpu.VMEM((2, 2, 64, 1024), BF),
            pltpu.VMEM((2, 64, 1024), BF),
            pltpu.VMEM((3, CH, 128), BF),
            dma((5,)), dma((2, 3)), dma((5,)), dma((16, 3)), dma((3, 3)), dma((3, 3)), dma((8, 3)),
            dma((3,)), dma((3,)), dma((8,)), dma((16,)), dma((2, 8)), dma((16,)), dma((2,)),
            dma((10, 6)), dma((16, 4)), dma((3,)), dma((3,)), dma((8,)), dma((8, 2)),
            dma((4,)), dma((4,)), dma((6,)), dma((4,)), dma((2,)), dma((12,)), dma((6,)),
        ],
        compiler_params=pltpu.CompilerParams(has_side_effects=True, collective_id=0, vmem_limit_bytes=60 * 1024 * 1024),
        cost_estimate=pl.CostEstimate(flops=8 * 10**9, bytes_accessed=10**8, transcendentals=10**7),
    )(*args)


def per_device(
    residual, query_small, key_small, value_small, query_large, key_large, value_large,
    lambda_small, lambda_large, head_gain, output_small, output_large, norm_gain,
    gate_weight, up_weight, down_weight,
):
    flat = lambda a: a.reshape(a.shape[0], a.shape[2])
    return block(
        flat(query_small), flat(query_large), flat(key_small), flat(key_large), flat(value_small),
        flat(value_large), lambda_small, lambda_large, head_gain.reshape(1, 128), output_small, output_large, residual,
        norm_gain.reshape(1, 2048), gate_weight.T, up_weight.T, down_weight,
    )


def solution(mesh):
    in_specs = (
        P(("sp", "tp"), None),
        P("sp", "tp", None), P("sp", "tp", None), P("sp", "tp", None),
        P("sp", "tp", None), P("sp", "tp", None), P("sp", "tp", None),
        P("tp"), P("tp"), P(), P("tp", None), P("tp", None), P(),
        P("sp", "tp"), P("sp", "tp"), P("tp", "sp"),
    )
    return jax.shard_map(
        per_device, mesh=mesh, in_specs=in_specs, out_specs=P(("sp", "tp"), None), check_vma=False
    )
```
